32 devices in a mesh: ep: 4 (over y, x), tp: 8 (over z, core).
Axes of the slice: x: 2, y: 2, z: 4, core: 2. Of those that a mesh axis runs over, the one named last changes fastest.
Arguments:
- receptance: bfloat16 [4096, 1024], P('ep', 'tp'), may hold values from -6 to 6
- key_in: bfloat16 [4096, 1024], P('ep', 'tp'), may hold values from -6 to 6
- payload_vectors: bfloat16 [4096, 1024], P('ep', 'tp'), may hold values from -6 to 6
- decay_in: bfloat16 [4096, 1024], P('ep', 'tp'), may hold values from -30 to 3
- rate_in: bfloat16 [4096, 1024], P('ep', 'tp'), may hold values from -30 to 6
- gate_in: bfloat16 [4096, 1024], P('ep', 'tp'), may hold values from -6 to 6
- norm_gain: float32 [1024], P('tp'), may hold values from 0.1 to 1.9
- out_weight: bfloat16 [1024, 2048], P('tp'), may hold values from -0.1875 to 0.1875
- moe_in: bfloat16 [4096, 2048], P(('ep', 'tp')), may hold values from -6 to 6
- moe_gain: float32 [2048], replicated, may hold values from 0.1 to 1.9
- routes: int32 [4096, 2], P(('ep', 'tp')), may hold values from 0 to 7, all different within a row; in each aligned block of 128 rows (0 to 127, 128 to 255, ...) at most 48 rows name the same one
- route_weights: float32 [4096, 2], P(('ep', 'tp')), may hold values from 0.2 to 1
- expert_gate: bfloat16 [8, 2048, 512], P('ep', None, 'tp'), may hold values from -0.125 to 0.125
- expert_up: bfloat16 [8, 2048, 512], P('ep', None, 'tp'), may hold values from -0.125 to 0.125
- expert_down: bfloat16 [8, 2048, 512], P('ep', None, 'tp'), may hold values from -0.25 to 0.25
- shared_gate: bfloat16 [2048, 512], replicated, may hold values from -0.125 to 0.125
- shared_up: bfloat16 [2048, 512], replicated, may hold values from -0.125 to 0.125
- shared_down: bfloat16 [512, 2048], replicated, may hold values from -0.25 to 0.25
Outputs:
- mixed: bfloat16 [4096, 2048], P(('ep', 'tp'))
- moe_out: bfloat16 [4096, 2048], P(('ep', 'tp'))
The draws below stay inside these ranges and needn't reach their ends.
Inputs may be any that keep to these rules, and one draw needn't show every extreme that they name: `routes`: each token names 2 different experts; within the rows of one device no expert is named more than 48 times, a bound that some block reaches there.
All inputs are finite; a program needn't handle non-finite values.
Results may differ from the reference program's by a relative error of at most 0.019.
Values may be sent and summed in bfloat16 or wider, within the bound.
A program may use at most 128 MiB of HBM per device.

```python
import math
import jax
import jax.numpy as jnp
import numpy as np
from jax import lax

D = 2048
MIX_WIDTH = 1024
HEAD_DIM = 64
HEADS = 16
BLOCK = 64
SEQ = 4096
MOE_TOKENS = 128
MOE_ALL = 4096
TOP_K = 2
EXPERTS = 8
EXPERT_WIDTH = 512
SHARED_WIDTH = 512
SLOTS = 48


def slow_channel_index(key):
    kinds = jax.random.randint(jax.random.fold_in(key, 11), (HEADS,), 0, 8)
    slow = kinds < 4
    return jnp.repeat(slow, HEAD_DIM)[None, :]


def draw_decay_in(key, part):
    slow = slow_channel_index(key)
    capacity_locations = jnp.arange(SEQ, dtype=jnp.int32)
    noise = jnp.clip(jax.random.normal(jax.random.fold_in(key, 1), (SEQ, MIX_WIDTH), jnp.float32), -2.0, 2.0) * 0.7
    spans = jax.random.uniform(jax.random.fold_in(key, 2), (16,), jnp.float32, -0.7, 0.7)
    shift = spans[capacity_locations * 16 // SEQ][:, None]
    channel = jax.random.uniform(jax.random.fold_in(key, 3), (MIX_WIDTH,), jnp.float32, 0.2, 0.6)[None, :]
    slow_value_rows = jnp.log(channel / SEQ) + 0.5
    fast_value = jnp.log(channel) - 2.6
    displacement_anchor = jnp.where(slow, slow_value_rows, fast_value) + shift + noise
    specialist_places = jax.random.randint(jax.random.fold_in(key, 4), (2,), 0, SEQ)
    contiguous_span_length = jnp.any(capacity_locations[:, None] == specialist_places[None, :], axis=1)[:, None]
    return jnp.where(contiguous_span_length, 1.5, displacement_anchor).astype(jnp.bfloat16)


def draw_rate_in(key, part):
    slow = slow_channel_index(key)
    noise = jnp.clip(jax.random.normal(jax.random.fold_in(key, 5), (SEQ, MIX_WIDTH), jnp.float32), -3.0, 3.0)
    slow_value_rows = jnp.log(jnp.float32(19.2) / SEQ) + 0.7 * noise
    return jnp.where(slow, slow_value_rows, noise).astype(jnp.bfloat16)


def block_scale(rng, shape, shards, least, largest):
    def one(position, shards_of):
        steps = jax.random.uniform(jax.random.fold_in(jax.random.fold_in(rng, 6), position), (shards_of,), jnp.float32, least / len(shards), largest / len(shards))
        return jnp.repeat(jnp.exp(steps), shape[position] // shards_of).reshape((-1,) + (1,) * (len(shape) - position - 1))

    level = one(*shards[0])
    for cut in shards[1:]:
        level = level * one(*cut)
    return level


def shared_out(key, own, number, rows, number_of, top, bound, slope):
    order = jax.random.permutation(key, number_of)
    heavy_load, ordinary = load_shares(number_of, rows * top, bound, slope, True), load_shares(number_of, rows * top, bound, slope, False)
    places = jnp.arange(number_of)

    def named(sizes, offset_by):
        used = int((sizes > 0).sum())
        fixed = max(1, used // 4)
        passed = fixed + (places - fixed + offset_by * (used - fixed)) % max(1, number_of - fixed)
        return jnp.zeros((number_of,), jnp.int32).at[order[jnp.where(places < fixed, places, passed)]].set(jnp.asarray(sizes, jnp.int32))

    sizes = jnp.where(number % 4 == 0, named(heavy_load, number // 4), named(ordinary, number - number // 4 - 1))
    mixed = jax.random.permutation(jax.random.fold_in(own, 3), number_of)
    source_of, receiver = mixed[0:number_of // 2 * 2:2], mixed[1:number_of // 2 * 2:2]
    room = jnp.minimum(sizes[source_of] - 1, bound - sizes[receiver]) // 2
    room = jnp.where((source_of == order[0]) | (receiver == order[0]) | (sizes[receiver] == 0), 0, jnp.maximum(room, 0))
    passed = jax.random.randint(jax.random.fold_in(own, 4), (number_of // 2,), 0, 1 << 20) % (room + 1)
    sizes = sizes.at[source_of].add(-passed).at[receiver].add(passed)
    members = jnp.searchsorted(jnp.cumsum(sizes), jnp.arange(rows * top), side="right").astype(jnp.int32)
    table = members.reshape(top, rows).T
    table = table[jax.random.permutation(jax.random.fold_in(own, 1), rows)]
    offset_by = jax.random.randint(jax.random.fold_in(own, 2), (rows, 1), 0, top)
    return jnp.take_along_axis(table, (jnp.arange(top)[None, :] + offset_by) % top, axis=1)


def load_shares(amount, total, bound, skew, full):
    loads = [(1 << 20) // math.isqrt(standing ** skew) + 1 for standing in range(1, amount + 1)]
    largest = bound if full else min(bound, max(-(-total // amount), total * loads[0] // sum(loads)))
    least = 1 if total - largest >= amount - 1 else 0
    holding, surplus = [largest] + [least] * (amount - 1), total - largest - least * (amount - 1)
    while surplus > 0:
        movable = [i for i in range(1, amount) if holding[i] < largest] or [i for i in range(1, amount) if holding[i] < bound]
        pool, remaining = sum([loads[i] for i in movable]), surplus
        for i in movable:
            more = min(bound - holding[i], max(1, remaining * loads[i] // pool), surplus)
            holding[i] = holding[i] + more
            surplus = surplus - more
    return np.array(holding)


def scatter_about(own_key, dims, width, reach, pieces=(), held_as=jnp.bfloat16):
    factor_of = block_scale(own_key, dims, pieces, -0.22, 0.18) if pieces else 1.0
    entries = jax.random.normal(own_key, dims, jnp.float32) * width * factor_of
    return jnp.minimum(jnp.maximum(entries, -reach), reach).astype(held_as)


def setup_inputs(seed: int = 0) -> dict:
    arg_keys = jax.random.split(jax.random.key(seed), 19)
    receptance = scatter_about(arg_keys[0], (SEQ, MIX_WIDTH), 1.0, 6.0, ((0, 4), (1, 8)))
    key_in = scatter_about(arg_keys[1], (SEQ, MIX_WIDTH), 1.0, 6.0, ((0, 4), (1, 8)))
    payload_vectors = scatter_about(arg_keys[2], (SEQ, MIX_WIDTH), 1.0, 6.0, ((0, 4), (1, 8)))
    decay_in = draw_decay_in(jax.random.fold_in(arg_keys[18], 71), 0)
    rate_in = draw_rate_in(jax.random.fold_in(arg_keys[18], 71), 0)
    gate_in = scatter_about(arg_keys[5], (SEQ, MIX_WIDTH), 1.0, 6.0, ((0, 4), (1, 8)))
    norm_gain = jnp.clip(1.0 + 0.18 * jax.random.normal(arg_keys[6], (MIX_WIDTH,), jnp.float32), 0.1, 1.9)
    out_weight = scatter_about(arg_keys[7], (MIX_WIDTH, D), MIX_WIDTH ** -0.5, 0.1875, ((0, 8),))
    moe_in = scatter_about(arg_keys[8], (MOE_ALL, D), 1.0, 6.0, ((0, 32),))
    moe_gain = jnp.clip(1.0 + 0.18 * jax.random.normal(arg_keys[9], (D,), jnp.float32), 0.1, 1.9)
    routes_keys = jax.random.split(jax.random.fold_in(arg_keys[10], 1), MOE_ALL // MOE_TOKENS)
    routes_turns = jax.random.permutation(jax.random.fold_in(arg_keys[10], 3), MOE_ALL // MOE_TOKENS)
    routes = jax.vmap(lambda own, number: shared_out(jax.random.fold_in(arg_keys[10], 2), own, number, MOE_TOKENS, EXPERTS, TOP_K, SLOTS, 1))(routes_keys, routes_turns).reshape((MOE_ALL, TOP_K))
    route_weights = jnp.clip(0.2 + 0.8 * jax.random.uniform(arg_keys[11], (MOE_ALL, TOP_K), jnp.float32) ** block_scale(arg_keys[11], (MOE_ALL, TOP_K), ((0, 32),), -0.2, 0.2), 0.2, 1.0)
    expert_gate = scatter_about(arg_keys[12], (EXPERTS, D, EXPERT_WIDTH), D ** -0.5, 0.125, ((0, 4), (2, 8)))
    expert_up = scatter_about(arg_keys[13], (EXPERTS, D, EXPERT_WIDTH), D ** -0.5, 0.125, ((0, 4), (2, 8)))
    expert_down = scatter_about(arg_keys[14], (EXPERTS, D, EXPERT_WIDTH), EXPERT_WIDTH ** -0.5, 0.25, ((0, 4), (2, 8)))
    shared_gate = scatter_about(arg_keys[15], (D, SHARED_WIDTH), D ** -0.5, 0.125)
    shared_up = scatter_about(arg_keys[16], (D, SHARED_WIDTH), D ** -0.5, 0.125)
    shared_down = scatter_about(arg_keys[17], (SHARED_WIDTH, D), SHARED_WIDTH ** -0.5, 0.25)
    return {"receptance": receptance, "key_in": key_in, "payload_vectors": payload_vectors, "decay_in": decay_in, "rate_in": rate_in, "gate_in": gate_in, "norm_gain": norm_gain, "out_weight": out_weight, "moe_in": moe_in, "moe_gain": moe_gain, "routes": routes, "route_weights": route_weights, "expert_gate": expert_gate, "expert_up": expert_up, "expert_down": expert_down, "shared_gate": shared_gate, "shared_up": shared_up, "shared_down": shared_down}


def mult(form, left, right):
    return jnp.einsum(form, left, right, precision=lax.Precision.HIGHEST)

def block_maps(receive, keys, values, log_decay, alpha, beta):
    length = receive.shape[-2]
    cumul = jnp.cumsum(log_decay, axis=-2)
    before = cumul - log_decay
    ending = cumul[..., -1:, :]
    query_dec = receive * jnp.exp(cumul)
    alpha_dec = alpha * jnp.exp(before)
    key_grow = keys * jnp.exp(-cumul)
    beta_grow = beta * jnp.exp(-cumul)
    row_index = jnp.arange(length, dtype=jnp.int32)[:, None]
    col_index = jnp.arange(length, dtype=jnp.int32)[None, :]
    strict = col_index < row_index
    inclusive_cumsum = col_index <= row_index
    couple = jnp.where(strict, mult('...tc,...sc->...ts', alpha_dec, beta_grow), 0.0)
    insert_term = jnp.where(strict, mult('...tc,...sc->...ts', alpha_dec, key_grow), 0.0)
    inverse = jnp.eye(length, dtype=jnp.float32) + couple
    power = couple
    for section in range(length.bit_length() - 2):
        power = mult('...ij,...jk->...ik', power, power)
        inverse = inverse + mult('...ij,...jk->...ik', inverse, power)
    q_rows = mult('...ts,...sc->...tc', inverse, alpha_dec)
    z_rows = mult('...ts,...sv->...tv', inverse, mult('...ts,...sv->...tv', insert_term, values))
    read_beta = jnp.where(inclusive_cumsum, mult('...tc,...sc->...ts', query_dec, beta_grow), 0.0)
    read_key = jnp.where(inclusive_cumsum, mult('...tc,...sc->...ts', query_dec, key_grow), 0.0)
    query_bar = query_dec + mult('...ts,...sc->...tc', read_beta, q_rows)
    local_out = mult('...ts,...sv->...tv', read_beta, z_rows) + mult('...ts,...sv->...tv', read_key, values)
    beta_end = beta * jnp.exp(ending - cumul)
    key_end = keys * jnp.exp(ending - cumul)
    eye = jnp.eye(keys.shape[-1], dtype=jnp.float32)
    carry_map = mult('...tc,...td->...cd', q_rows, beta_end) + jnp.exp(ending)[..., 0, :, None] * eye
    source_map = mult('...tv,...tk->...vk', z_rows, beta_end) + mult('...tv,...tk->...vk', values, key_end)
    return (query_bar, local_out, carry_map, source_map)

def mixer(receptance, key_in, payload_vectors, decay_in, rate_in, gate_in, norm_gain, out_weight):
    length = receptance.shape[0]

    def split_heads(array):
        return array.reshape(length // BLOCK, BLOCK, HEADS, HEAD_DIM).transpose(2, 0, 1, 3)
    keys = split_heads(key_in.astype(jnp.float32))
    unit = keys * lax.rsqrt(lax.optimization_barrier(jnp.sum(keys * keys, -1, keepdims=True)) + 1e-06)
    rate = split_heads(jax.nn.sigmoid(rate_in.astype(jnp.float32)))
    log_decay = split_heads(-jnp.exp(-jax.nn.softplus(-decay_in.astype(jnp.float32)) - 0.5))
    queries = split_heads(receptance.astype(jnp.float32))
    values = split_heads(payload_vectors.astype(jnp.float32))

    def one_head(operands):
        query_h, key_h, value_h, decay_h, alpha_h, beta_h = operands
        query_bar, local_out, carry_map, source_map = block_maps(query_h, key_h, value_h, decay_h, alpha_h, beta_h)

        def advance(state, blocks):
            bar_b, local_b, carry_b, source_b = blocks
            output = mult('tk,vk->tv', bar_b, state) + local_b
            return (mult('ij,jk->ik', state, carry_b) + source_b, output)
        start_state = jnp.zeros((HEAD_DIM, HEAD_DIM), jnp.float32)
        final, outputs = lax.scan(advance, start_state, (query_bar, local_out, carry_map, source_map))
        return outputs
    recur = lax.map(one_head, (queries, keys, values, log_decay, -unit, unit * rate))
    recur = recur.transpose(1, 2, 0, 3).reshape(length, HEADS, HEAD_DIM)
    centered = recur - lax.optimization_barrier(jnp.mean(recur, -1, keepdims=True))
    rescaled_input = centered * lax.rsqrt(lax.optimization_barrier(jnp.mean(centered * centered, -1, keepdims=True)) + 0.00064)
    gated = rescaled_input.reshape(length, MIX_WIDTH) * norm_gain * jax.nn.sigmoid(gate_in.astype(jnp.float32))
    mixer_rows = gated.astype(jnp.bfloat16)
    return jnp.dot(mixer_rows, out_weight, preferred_element_type=jnp.float32).astype(jnp.bfloat16)

def experts(moe_in, moe_gain, routes, route_weights, expert_gate, expert_up, expert_down, shared_gate, shared_up, shared_down):
    tile_rows = 128
    values = moe_in.astype(jnp.float32)
    centered = values - lax.optimization_barrier(jnp.mean(values, -1, keepdims=True))
    rescaled_input = (centered * lax.rsqrt(lax.optimization_barrier(jnp.mean(centered * centered, -1, keepdims=True)) + 1e-05) * moe_gain).astype(jnp.bfloat16)
    shared_gate_out = jnp.dot(rescaled_input, shared_gate, preferred_element_type=jnp.float32)
    shared_up_out = jnp.dot(rescaled_input, shared_up, preferred_element_type=jnp.float32)
    shared_hidden = (jax.nn.silu(shared_gate_out) * shared_up_out).astype(jnp.bfloat16)
    shared_term = jnp.dot(shared_hidden, shared_down, preferred_element_type=jnp.float32)
    share = 2.5 * route_weights / lax.optimization_barrier(jnp.sum(route_weights, -1, keepdims=True))
    tokens = rescaled_input.shape[0]
    pairs = tokens * TOP_K
    flat_expert = routes.reshape(-1).astype(jnp.int32)
    flat_token = jnp.repeat(jnp.arange(tokens, dtype=jnp.int32), TOP_K)
    flat_share = share.reshape(-1)
    order = jnp.argsort(flat_expert, stable=True).astype(jnp.int32)
    sorted_expert = flat_expert[order]
    counts = lax.optimization_barrier(jnp.sum((flat_expert[:, None] == jnp.arange(EXPERTS, dtype=jnp.int32)[None, :]).astype(jnp.int32), 0)).astype(jnp.int32)
    padded = ((counts + tile_rows - 1) // tile_rows * tile_rows).astype(jnp.int32)
    pad_end = jnp.cumsum(padded).astype(jnp.int32)
    pad_start = (pad_end - padded).astype(jnp.int32)
    first = (jnp.cumsum(counts) - counts).astype(jnp.int32)
    dest = (pad_start[sorted_expert] + jnp.arange(pairs, dtype=jnp.int32) - first[sorted_expert]).astype(jnp.int32)
    capacity = (pairs + tile_rows - 1) // tile_rows * tile_rows + EXPERTS * tile_rows
    blocks = capacity // tile_rows
    slot_token = jnp.full((capacity,), tokens, jnp.int32).at[dest].set(flat_token[order])
    slot_share = jnp.zeros((capacity,), jnp.float32).at[dest].set(flat_share[order])
    group_starts = jnp.arange(blocks, dtype=jnp.int32) * tile_rows
    block_expert = jnp.minimum(jnp.searchsorted(pad_end, group_starts, side='right').astype(jnp.int32), EXPERTS - 1).astype(jnp.int32)
    rows_padded = jnp.concatenate([rescaled_input, jnp.zeros((1, rescaled_input.shape[1]), jnp.bfloat16)], axis=0)

    def add_block(total, operands):
        token_ids, weights, expert = operands
        rows = rows_padded[token_ids]
        gate = jnp.dot(rows, expert_gate[expert], preferred_element_type=jnp.float32)
        upper = jnp.dot(rows, expert_up[expert], preferred_element_type=jnp.float32)
        hidden = (jax.nn.silu(gate) * upper).astype(jnp.bfloat16)
        result = jnp.dot(hidden, expert_down[expert].T, preferred_element_type=jnp.float32).astype(jnp.bfloat16)
        return (total.at[token_ids].add(result.astype(jnp.float32) * weights[:, None]), None)
    start_total = jnp.zeros((tokens + 1, rescaled_input.shape[1]), jnp.float32)
    total, unused = lax.scan(add_block, start_total, (slot_token.reshape(blocks, tile_rows), slot_share.reshape(blocks, tile_rows), block_expert))
    return (shared_term + total[:tokens]).astype(jnp.bfloat16)

def reference(receptance, key_in, payload_vectors, decay_in, rate_in, gate_in, norm_gain, out_weight, moe_in, moe_gain, routes, route_weights, expert_gate, expert_up, expert_down, shared_gate, shared_up, shared_down):
    mixed = mixer(receptance, key_in, payload_vectors, decay_in, rate_in, gate_in, norm_gain, out_weight)
    moe_out = experts(moe_in, moe_gain, routes, route_weights, expert_gate, expert_up, expert_down, shared_gate, shared_up, shared_down)
    return (mixed, moe_out)
```

```python
import functools

import jax
import jax.numpy as jnp
from jax import lax
from jax.experimental import pallas as pl
from jax.experimental.pallas import tpu as pltpu
from jax.sharding import PartitionSpec as P

HEAD_DIM = 64
BLOCK = 64


def dims(form):
    return {"nn": ((1,), (0,)), "nt": ((1,), (1,)), "tn": ((0,), (0,))}[form]


def mm1(left, right, form="nn"):
    return lax.dot_general(
        left.astype(jnp.bfloat16),
        right.astype(jnp.bfloat16),
        (dims(form), ((), ())),
        preferred_element_type=jnp.float32,
    )


def mm3(left, right, form="nn"):
    lh, rh = left.astype(jnp.bfloat16), right.astype(jnp.bfloat16)
    ll = (left - lh.astype(jnp.float32)).astype(jnp.bfloat16)
    rl = (right - rh.astype(jnp.float32)).astype(jnp.bfloat16)
    return mm1(lh, rh, form) + (mm1(lh, rl, form) + mm1(ll, rh, form))


mm_g = mm3
mm_inv = mm3
mm_q = mm3
mm_out = mm3
mm_car = mm3
mm_scan = mm3


def head_masks(rows, width):
    lane = lax.broadcasted_iota(jnp.int32, (rows, width), 1)
    return lane < HEAD_DIM


def stacked(x):
    first = head_masks(*x.shape)
    return jnp.concatenate([jnp.where(first, x, 0.0), jnp.where(first, 0.0, x)], axis=0)


def per_head_sum(x):
    first = head_masks(*x.shape)
    one = jnp.sum(jnp.where(first, x, 0.0), axis=-1, keepdims=True)
    both = jnp.sum(jnp.where(first, 0.0, x), axis=-1, keepdims=True)
    return jnp.where(first, one, both)


def sigmoid(x):
    return 1.0 / (1.0 + jnp.exp(-x))


def local_block(r_in, k_in, v_in, d_in, b_in):
    f32 = jnp.float32
    keys = k_in.astype(f32)
    unit = keys * lax.rsqrt(per_head_sum(keys * keys) + 1e-06)
    log_decay = sigmoid(d_in.astype(f32)) * -0.6065306597126334
    tri_row = lax.broadcasted_iota(jnp.int32, (BLOCK, 3 * BLOCK), 0)
    tri_col = lax.broadcasted_iota(jnp.int32, (BLOCK, 3 * BLOCK), 1) % BLOCK
    tri = jnp.where(tri_col <= tri_row, 1.0, 0.0).astype(jnp.bfloat16)
    hi = log_decay.astype(jnp.bfloat16)
    rest = log_decay - hi.astype(f32)
    mid = rest.astype(jnp.bfloat16)
    low = (rest - mid.astype(f32)).astype(jnp.bfloat16)
    cumul = mm1(tri, jnp.concatenate([hi, mid, low], axis=0))
    end_scale = jnp.exp(cumul[BLOCK - 1 :, :])
    shrink = jnp.exp(-cumul)
    query2 = stacked(r_in.astype(f32) * jnp.exp(cumul))
    alpha2 = stacked(-unit * jnp.exp(cumul - log_decay))
    key_grow = keys * shrink
    beta_grow = unit * sigmoid(b_in.astype(f32)) * shrink
    values2 = stacked(v_in.astype(f32))
    two = 2 * BLOCK
    grams = mm_g(
        jnp.concatenate([alpha2, query2], axis=0),
        jnp.concatenate([beta_grow, beta_grow, key_grow, key_grow], axis=0),
        "nt",
    )
    row = lax.broadcasted_iota(jnp.int32, (two, two), 0)
    col = lax.broadcasted_iota(jnp.int32, (two, two), 1)
    same = row // BLOCK == col // BLOCK
    strict = same & (col < row)
    inclusive = same & (col <= row)
    couple = jnp.where(strict, grams[:two, :two], 0.0)
    insert = jnp.where(strict, grams[:two, two:], 0.0)
    read_beta = jnp.where(inclusive, grams[two:, :two], 0.0)
    read_key = jnp.where(inclusive, grams[two:, two:], 0.0)
    size = 8
    near = jnp.where(row // size == col // size, couple, 0.0)
    inverse = jnp.where(row == col, 1.0, 0.0) + near
    power = mm_inv(near, near)
    both = mm_inv(jnp.concatenate([inverse, power], axis=0), power)
    inverse = inverse + both[:two]
    inverse = inverse + mm_inv(inverse, both[two:])
    while size < BLOCK:
        wide = 2 * size
        off = jnp.where(
            (row // wide == col // wide) & (row // size != col // size), couple, 0.0
        )
        inverse = inverse + mm_inv(inverse, mm_inv(off, inverse))
        size = wide
    inserted = mm_q(insert, values2)
    qz = mm_q(inverse, jnp.concatenate([alpha2, inserted], axis=1))
    lower = jnp.concatenate([jnp.zeros_like(values2), values2], axis=1)
    stack = jnp.concatenate([qz, lower], axis=0)
    reads = mm_out(jnp.concatenate([read_beta, read_key], axis=1), stack)
    query_bar = query2 + reads[:, :two]
    local_out = reads[:, two:]
    ends = jnp.concatenate([stacked(beta_grow * end_scale), stacked(key_grow * end_scale)], axis=0)
    maps = mm_car(stack, ends, "tn")
    return query_bar, local_out, maps, end_scale


def local_kernel(unroll, r_ref, k_ref, v_ref, d_ref, b_ref, qp_ref, lo_ref, total_ref, state):
    two = 2 * BLOCK
    row = lax.broadcasted_iota(jnp.int32, (2 * two, two), 0)
    col = lax.broadcasted_iota(jnp.int32, (2 * two, two), 1)
    state[...] = jnp.where(row == col, 1.0, 0.0)

    @pl.loop(0, r_ref.shape[0] // (BLOCK * unroll))
    def _(step):
        parts = []
        for u in range(unroll):
            rows = pl.ds(pl.multiple_of((step * unroll + u) * BLOCK, BLOCK), BLOCK)
            parts.append(
                local_block(
                    r_ref[rows, :], k_ref[rows, :], v_ref[rows, :], d_ref[rows, :], b_ref[rows, :]
                )
            )
        now = state[...]
        for u, (query_bar, local_out, maps, end_scale) in enumerate(parts):
            rows = pl.ds(pl.multiple_of((step * unroll + u) * BLOCK, BLOCK), BLOCK)
            out = mm_scan(query_bar, now, "nt")
            qp_ref[rows, :] = out[:BLOCK, :two] + out[BLOCK:, :two]
            lo = out[:, two:] + local_out
            lo_ref[rows, :] = lo[:BLOCK] + lo[BLOCK:]
            moved = mm_scan(now, maps[:two]) + now * end_scale
            now = jnp.concatenate([moved[:two], moved[two:] + maps[two:]], axis=0)
        state[...] = now

    carry, source = state[:two, :], state[two:, :]
    total_ref[0] = (carry[:BLOCK] + carry[BLOCK:]).astype(total_ref.dtype)
    total_ref[1] = (source[:BLOCK] + source[BLOCK:]).astype(total_ref.dtype)


def finish_kernel(groups, qp_ref, lo_ref, all_ref, here_ref, gate_ref, gain_ref, out_ref):
    two = 2 * BLOCK
    here = here_ref[0]
    entry = jnp.zeros((two, two), jnp.float32)
    for k in range(groups):
        carry = stacked(all_ref[k, 0].astype(jnp.float32))
        source = stacked(all_ref[k, 1].astype(jnp.float32))
        entry = jnp.where(k < here, mm3(entry, carry) + source, entry)
    tile = 256 if qp_ref.shape[0] % 256 == 0 else BLOCK

    @pl.loop(0, qp_ref.shape[0] // tile)
    def _(step):
        rows = pl.ds(pl.multiple_of(step * tile, tile), tile)
        recur = mm3(qp_ref[rows, :], entry, "nt") + lo_ref[rows, :]
        centered = recur - per_head_sum(recur) * (1.0 / HEAD_DIM)
        spread = per_head_sum(centered * centered) * (1.0 / HEAD_DIM)
        normed = centered * lax.rsqrt(spread + 0.00064)
        gated = normed * gain_ref[...] * sigmoid(gate_ref[rows, :].astype(jnp.float32))
        out_ref[rows, :] = gated.astype(out_ref.dtype)


def gated_rows(receptance, key_in, payload_vectors, decay_in, rate_in, gate_in, norm_gain):
    length, channels = receptance.shape
    groups = lax.axis_size("ep")
    wide = 2 * HEAD_DIM
    spare = -channels % wide
    pad = lambda x: jnp.pad(x, ((0, 0),) * (x.ndim - 1) + ((0, spare),)) if spare else x
    receptance, key_in, payload_vectors, decay_in, rate_in, gate_in, norm_gain = (
        pad(x)
        for x in (receptance, key_in, payload_vectors, decay_in, rate_in, gate_in, norm_gain)
    )
    pairs = (channels + spare) // wide
    vmem = pl.BlockSpec(memory_space=pltpu.VMEM)
    unroll = 4
    done = []
    for pair in range(pairs):
        cut = slice(pair * wide, (pair + 1) * wide)
        qp, lo, total = pl.pallas_call(
            functools.partial(local_kernel, unroll),
            out_shape=(
                jax.ShapeDtypeStruct((length, wide), jnp.float32),
                jax.ShapeDtypeStruct((length, wide), jnp.float32),
                jax.ShapeDtypeStruct((2, HEAD_DIM, wide), jnp.bfloat16),
            ),
            in_specs=[vmem] * 5,
            out_specs=(vmem, vmem, vmem),
            scratch_shapes=[pltpu.VMEM((2 * wide, wide), jnp.float32)],
            cost_estimate=pl.CostEstimate(
                flops=2 * length * wide * wide * 60, bytes_accessed=4 << 20, transcendentals=0
            ),
        )(
            receptance[:, cut],
            key_in[:, cut],
            payload_vectors[:, cut],
            decay_in[:, cut],
            rate_in[:, cut],
        )
        everything = lax.all_gather(total, "ep")
        done.append(
            pl.pallas_call(
                functools.partial(finish_kernel, groups),
                out_shape=jax.ShapeDtypeStruct((length, wide), jnp.bfloat16),
                in_specs=[vmem] * 3 + [pl.BlockSpec(memory_space=pltpu.SMEM)] + [vmem] * 2,
                out_specs=vmem,
                cost_estimate=pl.CostEstimate(
                    flops=2 * length * wide * wide * 4, bytes_accessed=2 << 20, transcendentals=0
                ),
            )(
                qp,
                lo,
                everything,
                lax.axis_index("ep").reshape(1).astype(jnp.int32),
                gate_in[:, cut],
                norm_gain[cut].reshape(1, wide),
            )
        )
    rows = done[0] if pairs == 1 else jnp.concatenate(done, axis=1)
    return rows[:, :channels]


def expert_layer(
    moe_in,
    moe_gain,
    routes,
    route_weights,
    expert_gate,
    expert_up,
    expert_down,
    shared_gate,
    shared_up,
    shared_down,
):
    tokens, width = moe_in.shape
    top_count = routes.shape[1]
    local_count = expert_gate.shape[0]
    groups = lax.axis_size("ep")
    experts = local_count * groups
    slots = max(2, 3 * tokens * top_count // (2 * experts))
    values = moe_in.astype(jnp.float32)
    centered = values - jnp.mean(values, -1, keepdims=True)
    rescaled_input = (
        centered * lax.rsqrt(jnp.mean(centered * centered, -1, keepdims=True) + 1e-05) * moe_gain
    ).astype(jnp.bfloat16)
    flat = routes.reshape(-1)
    picks = (flat[:, None] == jnp.arange(experts, dtype=jnp.int32)[None, :]).astype(jnp.int32)
    earlier = jnp.cumsum(picks, axis=0) - picks
    rank = jnp.sum(earlier * picks, axis=1)
    slot_index = flat % local_count * (groups * slots) + flat // local_count * slots + rank
    total_slots = local_count * groups * slots
    match = slot_index[:, None] == jnp.arange(total_slots, dtype=jnp.int32)[None, :]
    owner = jnp.arange(tokens * top_count, dtype=jnp.int32) // top_count
    slot_token = jnp.sum(jnp.where(match, owner[:, None], 0), axis=0)
    filled = jnp.any(match, axis=0)
    outgoing = jnp.where(filled[:, None], rescaled_input[slot_token], jnp.zeros((), jnp.bfloat16))
    outgoing = outgoing.reshape(local_count, groups, slots, width)
    arrived = lax.all_to_all(outgoing, "ep", split_axis=1, concat_axis=1, tiled=True).reshape(
        local_count, groups * slots, width
    )
    shared_gate_out = jnp.dot(rescaled_input, shared_gate, preferred_element_type=jnp.float32)
    shared_up_out = jnp.dot(rescaled_input, shared_up, preferred_element_type=jnp.float32)
    shared_hidden = (jax.nn.silu(shared_gate_out) * shared_up_out).astype(jnp.bfloat16)
    shared_term = jnp.dot(shared_hidden, shared_down, preferred_element_type=jnp.float32)
    gate_whole, up_whole, down_whole = (
        lax.all_gather(expert_gate, "tp", axis=2, tiled=True),
        lax.all_gather(expert_up, "tp", axis=2, tiled=True),
        lax.all_gather(expert_down, "tp", axis=2, tiled=True),
    )
    gate = jnp.einsum("erd,edf->erf", arrived, gate_whole, preferred_element_type=jnp.float32)
    upper = jnp.einsum("erd,edf->erf", arrived, up_whole, preferred_element_type=jnp.float32)
    hidden = (jax.nn.silu(gate) * upper).astype(jnp.bfloat16)
    results = jnp.einsum("erf,edf->erd", hidden, down_whole, preferred_element_type=jnp.float32)
    sending = results.astype(jnp.bfloat16).reshape(local_count, groups, slots, width)
    returned = lax.all_to_all(sending, "ep", split_axis=1, concat_axis=1, tiled=True).reshape(
        total_slots, width
    )
    picked = returned[slot_index].reshape(tokens, top_count, width)
    share = 2.5 * route_weights / jnp.sum(route_weights, -1, keepdims=True)
    combined = shared_term + jnp.sum(picked.astype(jnp.float32) * share[:, :, None], axis=1)
    return combined.astype(jnp.bfloat16)


def shards(
    receptance,
    key_in,
    payload_vectors,
    decay_in,
    rate_in,
    gate_in,
    norm_gain,
    out_weight,
    moe_in,
    moe_gain,
    routes,
    route_weights,
    expert_gate,
    expert_up,
    expert_down,
    shared_gate,
    shared_up,
    shared_down,
):
    mixer_rows = gated_rows(
        receptance, key_in, payload_vectors, decay_in, rate_in, gate_in, norm_gain
    )
    token_rows = lax.all_to_all(mixer_rows, "tp", split_axis=0, concat_axis=1, tiled=True)
    mixed = jnp.dot(
        token_rows,
        lax.all_gather(out_weight, "tp", axis=0, tiled=True),
        preferred_element_type=jnp.float32,
    )
    moe_out = expert_layer(
        moe_in,
        moe_gain,
        routes,
        route_weights,
        expert_gate,
        expert_up,
        expert_down,
        shared_gate,
        shared_up,
        shared_down,
    )
    return (mixed.astype(jnp.bfloat16), moe_out)


def solution(mesh):
    placed = (
        P("ep", "tp"),
        P("ep", "tp"),
        P("ep", "tp"),
        P("ep", "tp"),
        P("ep", "tp"),
        P("ep", "tp"),
        P("tp"),
        P("tp", None),
        P(("ep", "tp"), None),
        P(),
        P(("ep", "tp"), None),
        P(("ep", "tp"), None),
        P("ep", None, "tp"),
        P("ep", None, "tp"),
        P("ep", None, "tp"),
        P(),
        P(),
        P(),
    )
    return jax.shard_map(
        shards,
        mesh=mesh,
        in_specs=placed,
        out_specs=(P(("ep", "tp"), None), P(("ep", "tp"), None)),
        check_vma=False,
    )
```

```python
import functools

import jax
import jax.numpy as jnp
from jax import lax
from jax.experimental import pallas as pl
from jax.experimental.pallas import tpu as pltpu
from jax.sharding import PartitionSpec as P

HEAD_DIM = 64
BLOCK = 64


def dims(form):
    return {"nn": ((1,), (0,)), "nt": ((1,), (1,)), "tn": ((0,), (0,))}[form]


def mm1(left, right, form="nn"):
    return lax.dot_general(
        left.astype(jnp.bfloat16),
        right.astype(jnp.bfloat16),
        (dims(form), ((), ())),
        preferred_element_type=jnp.float32,
    )


def mm3(left, right, form="nn"):
    lh, rh = left.astype(jnp.bfloat16), right.astype(jnp.bfloat16)
    ll = (left - lh.astype(jnp.float32)).astype(jnp.bfloat16)
    rl = (right - rh.astype(jnp.float32)).astype(jnp.bfloat16)
    return mm1(lh, rh, form) + (mm1(lh, rl, form) + mm1(ll, rh, form))


mm_g = mm3
mm_inv = mm3
mm_q = mm3
mm_out = mm3
mm_car = mm3
mm_scan = mm3


def head_masks(rows, width):
    lane = lax.broadcasted_iota(jnp.int32, (rows, width), 1)
    return lane < HEAD_DIM


def stacked(x):
    first = head_masks(*x.shape)
    return jnp.concatenate([jnp.where(first, x, 0.0), jnp.where(first, 0.0, x)], axis=0)


def per_head_sum(x):
    first = head_masks(*x.shape)
    one = jnp.sum(jnp.where(first, x, 0.0), axis=-1, keepdims=True)
    both = jnp.sum(jnp.where(first, 0.0, x), axis=-1, keepdims=True)
    return jnp.where(first, one, both)


def sigmoid(x):
    return 1.0 / (1.0 + jnp.exp(-x))


def local_block(r_in, k_in, v_in, d_in, b_in):
    f32 = jnp.float32
    keys = k_in.astype(f32)
    unit = keys * lax.rsqrt(per_head_sum(keys * keys) + 1e-06)
    log_decay = sigmoid(d_in.astype(f32)) * -0.6065306597126334
    tri_row = lax.broadcasted_iota(jnp.int32, (BLOCK, 3 * BLOCK), 0)
    tri_col = lax.broadcasted_iota(jnp.int32, (BLOCK, 3 * BLOCK), 1) % BLOCK
    tri = jnp.where(tri_col <= tri_row, 1.0, 0.0).astype(jnp.bfloat16)
    hi = log_decay.astype(jnp.bfloat16)
    rest = log_decay - hi.astype(f32)
    mid = rest.astype(jnp.bfloat16)
    low = (rest - mid.astype(f32)).astype(jnp.bfloat16)
    cumul = mm1(tri, jnp.concatenate([hi, mid, low], axis=0))
    end_scale = jnp.exp(cumul[BLOCK - 1 :, :])
    shrink = jnp.exp(-cumul)
    query2 = stacked(r_in.astype(f32) * jnp.exp(cumul))
    alpha2 = stacked(-unit * jnp.exp(cumul - log_decay))
    key_grow = keys * shrink
    beta_grow = unit * sigmoid(b_in.astype(f32)) * shrink
    values2 = stacked(v_in.astype(f32))
    two = 2 * BLOCK
    grams = mm_g(
        jnp.concatenate([alpha2, query2], axis=0),
        jnp.concatenate([beta_grow, beta_grow, key_grow, key_grow], axis=0),
        "nt",
    )
    row = lax.broadcasted_iota(jnp.int32, (two, two), 0)
    col = lax.broadcasted_iota(jnp.int32, (two, two), 1)
    same = row // BLOCK == col // BLOCK
    strict = same & (col < row)
    inclusive = same & (col <= row)
    couple = jnp.where(strict, grams[:two, :two], 0.0)
    insert = jnp.where(strict, grams[:two, two:], 0.0)
    read_beta = jnp.where(inclusive, grams[two:, :two], 0.0)
    read_key = jnp.where(inclusive, grams[two:, two:], 0.0)
    size = 8
    near = jnp.where(row // size == col // size, couple, 0.0)
    inverse = jnp.where(row == col, 1.0, 0.0) + near
    power = mm_inv(near, near)
    both = mm_inv(jnp.concatenate([inverse, power], axis=0), power)
    inverse = inverse + both[:two]
    inverse = inverse + mm_inv(inverse, both[two:])
    while size < BLOCK:
        wide = 2 * size
        off = jnp.where(
            (row // wide == col // wide) & (row // size != col // size), couple, 0.0
        )
        inverse = inverse + mm_inv(inverse, mm_inv(off, inverse))
        size = wide
    inserted = mm_q(insert, values2)
    qz = mm_q(inverse, jnp.concatenate([alpha2, inserted], axis=1))
    lower = jnp.concatenate([jnp.zeros_like(values2), values2], axis=1)
    stack = jnp.concatenate([qz, lower], axis=0)
    reads = mm_out(jnp.concatenate([read_beta, read_key], axis=1), stack)
    query_bar = query2 + reads[:, :two]
    local_out = reads[:, two:]
    ends = jnp.concatenate([stacked(beta_grow * end_scale), stacked(key_grow * end_scale)], axis=0)
    maps = mm_car(stack, ends, "tn")
    return query_bar, local_out, maps, end_scale


def mixer_kernel(
    unroll,
    groups,
    ring,
    r_ref,
    k_ref,
    v_ref,
    d_ref,
    b_ref,
    gate_ref,
    gain_ref,
    weight_ref,
    token_ref,
    whole_ref,
    state,
    qp_ref,
    lo_ref,
    rows_ref,
    totals,
    ring_send,
    ring_recv,
    pair_send,
    pair_recv,
    ep_send,
    ep_recv,
    row_send,
    row_recv,
    own_sem,
):
    two = 2 * BLOCK
    peers = 2 * ring
    here, mine = lax.axis_index("ep"), lax.axis_index("tp")
    depth, core = mine // 2, mine % 2
    partner = depth * 2 + 1 - core
    after = (depth + 1) % ring * 2 + core
    before = (depth + ring - 1) % ring * 2 + core
    chunks, height = weight_ref.shape[0], weight_ref.shape[1]
    kinds = chunks // 2
    span = peers * height
    tokens = token_ref.shape[0]
    MESH = pl.DeviceIdType.MESH

    def place(chunk, origin):
        last = chunk // (chunks - 2)
        base = (1 - last) * (chunk * span + origin * height) + last * (
            (chunks - 2) * span + origin * 2 * height + (chunk - chunks + 2) * height
        )
        return whole_ref.at[pl.ds(pl.multiple_of(base, height), height), :]

    def ring_copy(source, chunk, origin, step, target):
        return pltpu.make_async_remote_copy(
            src_ref=source,
            dst_ref=place(chunk, origin),
            send_sem=ring_send.at[chunk, step],
            recv_sem=ring_recv.at[chunk, step],
            device_id={"tp": target},
            device_id_type=MESH,
        )

    def pair_copy(source, chunk, origin, step):
        return pltpu.make_async_remote_copy(
            src_ref=source,
            dst_ref=place(chunk, origin),
            send_sem=pair_send.at[chunk, step],
            recv_sem=pair_recv.at[chunk, step],
            device_id={"tp": partner},
            device_id_type=MESH,
        )

    def own_copy(chunk):
        return pltpu.make_async_copy(
            weight_ref.at[chunk], place(chunk, mine), own_sem.at[chunk]
        )

    barrier = pltpu.get_barrier_semaphore()
    for q in range(1, peers):
        pl.semaphore_signal(
            barrier, inc=1, device_id={"tp": (mine + q) % peers}, device_id_type=MESH
        )
    for q in range(1, groups):
        pl.semaphore_signal(
            barrier, inc=1, device_id={"ep": (here + q) % groups}, device_id_type=MESH
        )
    pl.semaphore_wait(barrier, peers + groups - 2)

    def begin(kind, carry):
        for way, target in ((0, after), (1, before)):
            chunk = kind * 2 + way
            ring_copy(weight_ref.at[chunk], chunk, mine, 0, target).start()
            pair_copy(weight_ref.at[chunk], chunk, mine, 0).start()
            own_copy(chunk).start()
        return carry

    lax.fori_loop(0, kinds, begin, 0)

    def relay(k, carry):
        hop, kind = k // kinds + 1, k % kinds
        for way, target in ((0, after), (1, before)):
            chunk = kind * 2 + way
            shift = ring - hop if way == 0 else hop
            origin = (depth + shift) % ring * 2 + core
            block = place(chunk, origin)
            ring_copy(block, chunk, origin, hop - 1, target).wait_recv()

            @pl.when(hop < ring - 1)
            def _():
                ring_copy(block, chunk, origin, hop, target).start()

            pair_copy(block, chunk, origin, hop).start()
        return carry

    row = lax.broadcasted_iota(jnp.int32, (2 * two, two), 0)
    col = lax.broadcasted_iota(jnp.int32, (2 * two, two), 1)
    state[...] = jnp.where(row == col, 1.0, 0.0)
    turns = r_ref.shape[0] // (BLOCK * unroll)
    relays = (ring - 1) * kinds
    each = 2
    inside = min(turns, relays // each)

    def turn(step, carry):
        parts = []
        for u in range(unroll):
            rows = pl.ds(pl.multiple_of((step * unroll + u) * BLOCK, BLOCK), BLOCK)
            parts.append(
                local_block(
                    r_ref[rows, :], k_ref[rows, :], v_ref[rows, :], d_ref[rows, :], b_ref[rows, :]
                )
            )
        now = state[...]
        for u, (query_bar, local_out, maps, end_scale) in enumerate(parts):
            rows = pl.ds(pl.multiple_of((step * unroll + u) * BLOCK, BLOCK), BLOCK)
            out = mm_scan(query_bar, now, "nt")
            qp_ref[rows, :] = out[:BLOCK, :two] + out[BLOCK:, :two]
            lo = out[:, two:] + local_out
            lo_ref[rows, :] = lo[:BLOCK] + lo[BLOCK:]
            moved = mm_scan(now, maps[:two]) + now * end_scale
            now = jnp.concatenate([moved[:two], moved[two:] + maps[two:]], axis=0)
        state[...] = now

        @pl.when(step < inside)
        def _():
            lax.fori_loop(step * each, (step + 1) * each, relay, 0)

        return carry

    lax.fori_loop(0, turns, turn, 0)

    carry_map, source_map = state[:two, :], state[two:, :]
    totals[here, 0] = (carry_map[:BLOCK] + carry_map[BLOCK:]).astype(totals.dtype)
    totals[here, 1] = (source_map[:BLOCK] + source_map[BLOCK:]).astype(totals.dtype)

    def ep_copy(q, slot):
        return pltpu.make_async_remote_copy(
            src_ref=totals.at[slot],
            dst_ref=totals.at[slot],
            send_sem=ep_send.at[q],
            recv_sem=ep_recv.at[q],
            device_id={"ep": (here + q) % groups},
            device_id_type=MESH,
        )

    for q in range(1, groups):
        ep_copy(q, here).start()
    for q in range(1, groups):
        ep_copy(q, (here + groups - q) % groups).wait_recv()

    def enter(k, entry):
        carry = stacked(totals[k, 0].astype(jnp.float32))
        source = stacked(totals[k, 1].astype(jnp.float32))
        reached = jnp.where(k < here, 1.0, 0.0)
        return entry + reached * (mm3(entry, carry) + source - entry)

    entry = lax.fori_loop(0, groups, enter, jnp.zeros((two, two), jnp.float32))
    entry = entry.astype(jnp.float32)

    def row_copy(q, target, source):
        return pltpu.make_async_remote_copy(
            src_ref=rows_ref.at[pl.ds(pl.multiple_of(target * tokens, tokens), tokens), :],
            dst_ref=token_ref.at[:, pl.ds(pl.multiple_of(source * two, two), two)],
            send_sem=row_send.at[q],
            recv_sem=row_recv.at[q],
            device_id={"tp": target},
            device_id_type=MESH,
        )

    def finish(rows):
        recur = mm3(qp_ref[rows, :], entry, "nt") + lo_ref[rows, :]
        centered = recur - per_head_sum(recur) * (1.0 / HEAD_DIM)
        spread = per_head_sum(centered * centered) * (1.0 / HEAD_DIM)
        normed = centered * lax.rsqrt(spread + 0.00064)
        gated = normed * gain_ref[...] * sigmoid(gate_ref[rows, :].astype(jnp.float32))
        rows_ref[rows, :] = gated.astype(rows_ref.dtype)

    def finish_turn(q, carry):
        target = (mine + q) % peers
        finish(pl.ds(pl.multiple_of(target * tokens, tokens), tokens))
        return carry

    lax.fori_loop(0, peers, finish_turn, 0)
    own = rows_ref.at[pl.ds(pl.multiple_of(mine * tokens, tokens), tokens), :]
    own_rows = pltpu.make_async_copy(
        own, token_ref.at[:, pl.ds(pl.multiple_of(mine * two, two), two)], own_sem.at[chunks]
    )
    own_rows.start()

    def row_start(q, carry):
        row_copy(q, (mine + q) % peers, mine).start()
        return carry

    lax.fori_loop(1, peers, row_start, 0)

    lax.fori_loop(inside * each, relays, relay, 0)

    def close(chunk, carry):
        own_copy(chunk).wait()

        def shut(hop, inner):
            pair_copy(weight_ref.at[chunk], chunk, mine, hop).wait()
            return inner

        def shut_ring(hop, inner):
            ring_copy(weight_ref.at[chunk], chunk, mine, hop, after).wait_send()
            return inner

        lax.fori_loop(0, ring, shut, 0)
        lax.fori_loop(0, ring - 1, shut_ring, 0)
        return carry

    lax.fori_loop(0, chunks, close, 0)
    own_rows.wait()

    def row_end(q, carry):
        row_copy(q, (mine + q) % peers, (mine + peers - q) % peers).wait()
        return carry

    lax.fori_loop(1, peers, row_end, 0)
    for q in range(1, groups):
        ep_copy(q, here).wait_send()


def mixer_and_weights(
    receptance, key_in, payload_vectors, decay_in, rate_in, gate_in, norm_gain, weights
):
    length, channels = receptance.shape
    groups, peers = lax.axis_size("ep"), lax.axis_size("tp")
    ring = peers // 2
    wide = 2 * HEAD_DIM
    spare = wide - channels
    pad = lambda x: jnp.pad(x, ((0, 0),) * (x.ndim - 1) + ((0, spare),)) if spare else x
    chunks, height, width = weights.shape
    vmem = pl.BlockSpec(memory_space=pltpu.VMEM)
    dma = pltpu.SemaphoreType.DMA
    tokens, whole = pl.pallas_call(
        functools.partial(mixer_kernel, 4, groups, ring),
        out_shape=(
            jax.ShapeDtypeStruct((length // peers, peers * wide), jnp.bfloat16),
            jax.ShapeDtypeStruct((chunks * peers * height, width), jnp.bfloat16),
        ),
        in_specs=[vmem] * 8,
        out_specs=(vmem, pl.BlockSpec(memory_space=pl.ANY)),
        scratch_shapes=[
            pltpu.VMEM((2 * wide, wide), jnp.float32),
            pltpu.VMEM((length, wide), jnp.float32),
            pltpu.VMEM((length, wide), jnp.float32),
            pltpu.VMEM((length, wide), jnp.bfloat16),
            pltpu.VMEM((groups, 2, HEAD_DIM, wide), jnp.bfloat16),
            dma((chunks, ring)),
            dma((chunks, ring)),
            dma((chunks, ring)),
            dma((chunks, ring)),
            dma((groups,)),
            dma((groups,)),
            dma((peers,)),
            dma((peers,)),
            dma((chunks + 1,)),
        ],
        compiler_params=pltpu.CompilerParams(collective_id=0, has_side_effects=True),
        cost_estimate=pl.CostEstimate(
            flops=2 * length * wide * wide * 200, bytes_accessed=32 << 20, transcendentals=0
        ),
    )(
        pad(receptance),
        pad(key_in),
        pad(payload_vectors),
        pad(decay_in),
        pad(rate_in),
        pad(gate_in),
        pad(norm_gain).reshape(1, wide),
        weights,
    )
    if spare:
        tokens = tokens.reshape(-1, peers, wide)[:, :, :channels].reshape(-1, peers * channels)
    return tokens, whole


def expert_layer(
    moe_in,
    moe_gain,
    routes,
    route_weights,
    local_count,
    whole,
    shared_gate,
    shared_up,
    shared_down,
):
    tokens, width = moe_in.shape
    top_count = routes.shape[1]
    groups = lax.axis_size("ep")
    experts = local_count * groups
    slots = max(2, 3 * tokens * top_count // (2 * experts))
    values = moe_in.astype(jnp.float32)
    centered = values - jnp.mean(values, -1, keepdims=True)
    rescaled_input = (
        centered * lax.rsqrt(jnp.mean(centered * centered, -1, keepdims=True) + 1e-05) * moe_gain
    ).astype(jnp.bfloat16)
    flat = routes.reshape(-1)
    picks = (flat[:, None] == jnp.arange(experts, dtype=jnp.int32)[None, :]).astype(jnp.int32)
    earlier = jnp.cumsum(picks, axis=0) - picks
    rank = jnp.sum(earlier * picks, axis=1)
    slot_index = flat % local_count * (groups * slots) + flat // local_count * slots + rank
    total_slots = local_count * groups * slots
    match = slot_index[:, None] == jnp.arange(total_slots, dtype=jnp.int32)[None, :]
    owner = jnp.arange(tokens * top_count, dtype=jnp.int32) // top_count
    slot_token = jnp.sum(jnp.where(match, owner[:, None], 0), axis=0)
    filled = jnp.any(match, axis=0)
    outgoing = jnp.where(filled[:, None], rescaled_input[slot_token], jnp.zeros((), jnp.bfloat16))
    outgoing = outgoing.reshape(local_count, groups, slots, width)
    arrived = lax.all_to_all(outgoing, "ep", split_axis=1, concat_axis=1, tiled=True).reshape(
        local_count, groups * slots, width
    )
    shared_gate_out = jnp.dot(rescaled_input, shared_gate, preferred_element_type=jnp.float32)
    shared_up_out = jnp.dot(rescaled_input, shared_up, preferred_element_type=jnp.float32)
    shared_hidden = (jax.nn.silu(shared_gate_out) * shared_up_out).astype(jnp.bfloat16)
    shared_term = jnp.dot(shared_hidden, shared_down, preferred_element_type=jnp.float32)
    gate_whole, up_whole, down_whole = whole
    gate = jnp.einsum("erd,efd->erf", arrived, gate_whole, preferred_element_type=jnp.float32)
    upper = jnp.einsum("erd,efd->erf", arrived, up_whole, preferred_element_type=jnp.float32)
    hidden = (jax.nn.silu(gate) * upper).astype(jnp.bfloat16)
    results = jnp.einsum("erf,efd->erd", hidden, down_whole, preferred_element_type=jnp.float32)
    sending = results.astype(jnp.bfloat16).reshape(local_count, groups, slots, width)
    returned = lax.all_to_all(sending, "ep", split_axis=1, concat_axis=1, tiled=True).reshape(
        total_slots, width
    )
    picked = returned[slot_index].reshape(tokens, top_count, width)
    share = 2.5 * route_weights / jnp.sum(route_weights, -1, keepdims=True)
    combined = shared_term + jnp.sum(picked.astype(jnp.float32) * share[:, :, None], axis=1)
    return combined.astype(jnp.bfloat16)


def shards(
    receptance,
    key_in,
    payload_vectors,
    decay_in,
    rate_in,
    gate_in,
    norm_gain,
    out_weight,
    moe_in,
    moe_gain,
    routes,
    route_weights,
    expert_gate,
    expert_up,
    expert_down,
    shared_gate,
    shared_up,
    shared_down,
):
    local_count, width, part = expert_gate.shape
    weights = jnp.concatenate(
        [jnp.swapaxes(w, 1, 2) for w in (expert_gate, expert_up, expert_down)]
        + [out_weight.reshape(2, part, width)],
        axis=0,
    )
    token_rows, whole = mixer_and_weights(
        receptance, key_in, payload_vectors, decay_in, rate_in, gate_in, norm_gain, weights
    )
    whole = whole.reshape(4, -1, width)
    mixed = jnp.dot(token_rows, whole[3], preferred_element_type=jnp.float32)
    moe_out = expert_layer(
        moe_in,
        moe_gain,
        routes,
        route_weights,
        local_count,
        [whole[k].reshape(local_count, -1, width) for k in range(3)],
        shared_gate,
        shared_up,
        shared_down,
    )
    return (mixed.astype(jnp.bfloat16), moe_out)


def solution(mesh):
    placed = (
        P("ep", "tp"),
        P("ep", "tp"),
        P("ep", "tp"),
        P("ep", "tp"),
        P("ep", "tp"),
        P("ep", "tp"),
        P("tp"),
        P("tp", None),
        P(("ep", "tp"), None),
        P(),
        P(("ep", "tp"), None),
        P(("ep", "tp"), None),
        P("ep", None, "tp"),
        P("ep", None, "tp"),
        P("ep", None, "tp"),
        P(),
        P(),
        P(),
    )
    return jax.shard_map(
        shards,
        mesh=mesh,
        in_specs=placed,
        out_specs=(P(("ep", "tp"), None), P(("ep", "tp"), None)),
        check_vma=False,
    )
```

```python
import functools

import jax
import jax.numpy as jnp
from jax import lax
from jax.experimental import pallas as pl
from jax.experimental.pallas import tpu as pltpu
from jax.sharding import PartitionSpec as P

HEAD_DIM = 64
BLOCK = 64


def dims(form):
    return {"nn": ((1,), (0,)), "nt": ((1,), (1,)), "tn": ((0,), (0,))}[form]


def mm1(left, right, form="nn"):
    return lax.dot_general(
        left.astype(jnp.bfloat16),
        right.astype(jnp.bfloat16),
        (dims(form), ((), ())),
        preferred_element_type=jnp.float32,
    )


def mm3(left, right, form="nn"):
    lh, rh = left.astype(jnp.bfloat16), right.astype(jnp.bfloat16)
    ll = (left - lh.astype(jnp.float32)).astype(jnp.bfloat16)
    rl = (right - rh.astype(jnp.float32)).astype(jnp.bfloat16)
    return mm1(lh, rh, form) + (mm1(lh, rl, form) + mm1(ll, rh, form))


mm_g = mm3
mm_inv = mm3
mm_q = mm3
mm_out = mm3
mm_car = mm3
mm_scan = mm3


def head_masks(rows, width):
    lane = lax.broadcasted_iota(jnp.int32, (rows, width), 1)
    return lane < HEAD_DIM


def stacked(x):
    first = head_masks(*x.shape)
    return jnp.concatenate([jnp.where(first, x, 0.0), jnp.where(first, 0.0, x)], axis=0)


def per_head_sum(x):
    first = head_masks(*x.shape)
    one = jnp.sum(jnp.where(first, x, 0.0), axis=-1, keepdims=True)
    both = jnp.sum(jnp.where(first, 0.0, x), axis=-1, keepdims=True)
    return jnp.where(first, one, both)


def sigmoid(x):
    return 1.0 / (1.0 + jnp.exp(-x))


def local_block(r_in, k_in, v_in, d_in, b_in):
    f32 = jnp.float32
    keys = k_in.astype(f32)
    unit = keys * lax.rsqrt(per_head_sum(keys * keys) + 1e-06)
    log_decay = sigmoid(d_in.astype(f32)) * -0.6065306597126334
    tri_row = lax.broadcasted_iota(jnp.int32, (BLOCK, 3 * BLOCK), 0)
    tri_col = lax.broadcasted_iota(jnp.int32, (BLOCK, 3 * BLOCK), 1) % BLOCK
    tri = jnp.where(tri_col <= tri_row, 1.0, 0.0).astype(jnp.bfloat16)
    hi = log_decay.astype(jnp.bfloat16)
    rest = log_decay - hi.astype(f32)
    mid = rest.astype(jnp.bfloat16)
    low = (rest - mid.astype(f32)).astype(jnp.bfloat16)
    cumul = mm1(tri, jnp.concatenate([hi, mid, low], axis=0))
    end_scale = jnp.exp(cumul[BLOCK - 1 :, :])
    shrink = jnp.exp(-cumul)
    query2 = stacked(r_in.astype(f32) * jnp.exp(cumul))
    alpha2 = stacked(-unit * jnp.exp(cumul - log_decay))
    key_grow = keys * shrink
    beta_grow = unit * sigmoid(b_in.astype(f32)) * shrink
    values2 = stacked(v_in.astype(f32))
    two = 2 * BLOCK
    grams = mm_g(
        jnp.concatenate([alpha2, query2], axis=0),
        jnp.concatenate([beta_grow, beta_grow, key_grow, key_grow], axis=0),
        "nt",
    )
    row = lax.broadcasted_iota(jnp.int32, (two, two), 0)
    col = lax.broadcasted_iota(jnp.int32, (two, two), 1)
    same = row // BLOCK == col // BLOCK
    strict = same & (col < row)
    inclusive = same & (col <= row)
    couple = jnp.where(strict, grams[:two, :two], 0.0)
    insert = jnp.where(strict, grams[:two, two:], 0.0)
    read_beta = jnp.where(inclusive, grams[two:, :two], 0.0)
    read_key = jnp.where(inclusive, grams[two:, two:], 0.0)
    size = 8
    near = jnp.where(row // size == col // size, couple, 0.0)
    inverse = jnp.where(row == col, 1.0, 0.0) + near
    power = mm_inv(near, near)
    both = mm_inv(jnp.concatenate([inverse, power], axis=0), power)
    inverse = inverse + both[:two]
    inverse = inverse + mm_inv(inverse, both[two:])
    while size < BLOCK:
        wide = 2 * size
        off = jnp.where(
            (row // wide == col // wide) & (row // size != col // size), couple, 0.0
        )
        inverse = inverse + mm_inv(inverse, mm_inv(off, inverse))
        size = wide
    inserted = mm_q(insert, values2)
    qz = mm_q(inverse, jnp.concatenate([alpha2, inserted], axis=1))
    lower = jnp.concatenate([jnp.zeros_like(values2), values2], axis=1)
    stack = jnp.concatenate([qz, lower], axis=0)
    reads = mm_out(jnp.concatenate([read_beta, read_key], axis=1), stack)
    query_bar = query2 + reads[:, :two]
    local_out = reads[:, two:]
    ends = jnp.concatenate([stacked(beta_grow * end_scale), stacked(key_grow * end_scale)], axis=0)
    maps = mm_car(stack, ends, "tn")
    return query_bar, local_out, maps, end_scale


def mixer_kernel(
    unroll,
    groups,
    ring,
    r_ref,
    k_ref,
    v_ref,
    d_ref,
    b_ref,
    gate_ref,
    gain_ref,
    weight_ref,
    token_ref,
    whole_ref,
    state,
    qp_ref,
    lo_ref,
    rows_ref,
    totals,
    ring_send,
    ring_recv,
    pair_send,
    pair_recv,
    ep_send,
    ep_recv,
    row_send,
    row_recv,
    own_sem,
):
    two = 2 * BLOCK
    peers = 2 * ring
    here, mine = lax.axis_index("ep"), lax.axis_index("tp")
    depth, core = mine // 2, mine % 2
    partner = depth * 2 + 1 - core
    after = (depth + 1) % ring * 2 + core
    before = (depth + ring - 1) % ring * 2 + core
    chunks, height = weight_ref.shape[0], weight_ref.shape[1]
    kinds = chunks // 2
    span = peers * height
    tokens = token_ref.shape[0]
    MESH = pl.DeviceIdType.MESH

    def place(chunk, origin):
        last = chunk // (chunks - 2)
        base = (1 - last) * (chunk * span + origin * height) + last * (
            (chunks - 2) * span + origin * 2 * height + (chunk - chunks + 2) * height
        )
        return whole_ref.at[pl.ds(pl.multiple_of(base, height), height), :]

    def ring_copy(source, chunk, origin, step, target):
        return pltpu.make_async_remote_copy(
            src_ref=source,
            dst_ref=place(chunk, origin),
            send_sem=ring_send.at[chunk, step],
            recv_sem=ring_recv.at[chunk, step],
            device_id={"tp": target},
            device_id_type=MESH,
        )

    def pair_copy(source, chunk, origin, step):
        return pltpu.make_async_remote_copy(
            src_ref=source,
            dst_ref=place(chunk, origin),
            send_sem=pair_send.at[chunk, step],
            recv_sem=pair_recv.at[chunk, step],
            device_id={"tp": partner},
            device_id_type=MESH,
        )

    def own_copy(chunk):
        return pltpu.make_async_copy(
            weight_ref.at[chunk], place(chunk, mine), own_sem.at[chunk]
        )

    barrier = pltpu.get_barrier_semaphore()
    for q in range(1, peers):
        pl.semaphore_signal(
            barrier, inc=1, device_id={"tp": (mine + q) % peers}, device_id_type=MESH
        )
    for q in range(1, groups):
        pl.semaphore_signal(
            barrier, inc=1, device_id={"ep": (here + q) % groups}, device_id_type=MESH
        )
    pl.semaphore_wait(barrier, peers + groups - 2)

    def begin(kind, carry):
        for way, target in ((0, after), (1, before)):
            chunk = kind * 2 + way
            ring_copy(weight_ref.at[chunk], chunk, mine, 0, target).start()
            pair_copy(weight_ref.at[chunk], chunk, mine, 0).start()
            own_copy(chunk).start()
        return carry

    lax.fori_loop(0, kinds, begin, 0)

    def relay(k, carry):
        hop, kind = k // kinds + 1, k % kinds
        for way, target in ((0, after), (1, before)):
            chunk = kind * 2 + way
            shift = ring - hop if way == 0 else hop
            origin = (depth + shift) % ring * 2 + core
            block = place(chunk, origin)
            ring_copy(block, chunk, origin, hop - 1, target).wait_recv()

            @pl.when(hop < ring - 1)
            def _():
                ring_copy(block, chunk, origin, hop, target).start()

            pair_copy(block, chunk, origin, hop).start()
        return carry

    row = lax.broadcasted_iota(jnp.int32, (2 * two, two), 0)
    col = lax.broadcasted_iota(jnp.int32, (2 * two, two), 1)
    state[...] = jnp.where(row == col, 1.0, 0.0)
    turns = r_ref.shape[0] // (BLOCK * unroll)
    relays = (ring - 1) * kinds
    each = 2
    inside = min(turns, relays // each)

    def turn(step, carry):
        parts = []
        for u in range(unroll):
            rows = pl.ds(pl.multiple_of((step * unroll + u) * BLOCK, BLOCK), BLOCK)
            parts.append(
                local_block(
                    r_ref[rows, :], k_ref[rows, :], v_ref[rows, :], d_ref[rows, :], b_ref[rows, :]
                )
            )
        now = state[...]
        for u, (query_bar, local_out, maps, end_scale) in enumerate(parts):
            rows = pl.ds(pl.multiple_of((step * unroll + u) * BLOCK, BLOCK), BLOCK)
            out = mm_scan(query_bar, now, "nt")
            qp_ref[rows, :] = out[:BLOCK, :two] + out[BLOCK:, :two]
            lo = out[:, two:] + local_out
            lo_ref[rows, :] = lo[:BLOCK] + lo[BLOCK:]
            moved = mm_scan(now, maps[:two]) + now * end_scale
            now = jnp.concatenate([moved[:two], moved[two:] + maps[two:]], axis=0)
        state[...] = now

        @pl.when(step < inside)
        def _():
            lax.fori_loop(step * each, (step + 1) * each, relay, 0)

        return carry

    lax.fori_loop(0, turns, turn, 0)

    carry_map, source_map = state[:two, :], state[two:, :]
    totals[here, 0] = (carry_map[:BLOCK] + carry_map[BLOCK:]).astype(totals.dtype)
    totals[here, 1] = (source_map[:BLOCK] + source_map[BLOCK:]).astype(totals.dtype)

    def ep_copy(q, slot):
        return pltpu.make_async_remote_copy(
            src_ref=totals.at[slot],
            dst_ref=totals.at[slot],
            send_sem=ep_send.at[q],
            recv_sem=ep_recv.at[q],
            device_id={"ep": (here + q) % groups},
            device_id_type=MESH,
        )

    for q in range(1, groups):
        ep_copy(q, here).start()
    for q in range(1, groups):
        ep_copy(q, (here + groups - q) % groups).wait_recv()

    def enter(k, entry):
        carry = stacked(totals[k, 0].astype(jnp.float32))
        source = stacked(totals[k, 1].astype(jnp.float32))
        reached = jnp.where(k < here, 1.0, 0.0)
        return entry + reached * (mm3(entry, carry) + source - entry)

    entry = lax.fori_loop(0, groups, enter, jnp.zeros((two, two), jnp.float32))
    entry = entry.astype(jnp.float32)

    def row_copy(q, target, source):
        return pltpu.make_async_remote_copy(
            src_ref=rows_ref.at[pl.ds(pl.multiple_of(target * tokens, tokens), tokens), :],
            dst_ref=token_ref.at[:, pl.ds(pl.multiple_of(source * two, two), two)],
            send_sem=row_send.at[q],
            recv_sem=row_recv.at[q],
            device_id={"tp": target},
            device_id_type=MESH,
        )

    def finish(rows):
        recur = mm3(qp_ref[rows, :], entry, "nt") + lo_ref[rows, :]
        centered = recur - per_head_sum(recur) * (1.0 / HEAD_DIM)
        spread = per_head_sum(centered * centered) * (1.0 / HEAD_DIM)
        normed = centered * lax.rsqrt(spread + 0.00064)
        gated = normed * gain_ref[...] * sigmoid(gate_ref[rows, :].astype(jnp.float32))
        rows_ref[rows, :] = gated.astype(rows_ref.dtype)

    def finish_turn(q, carry):
        target = (mine + q) % peers
        finish(pl.ds(pl.multiple_of(target * tokens, tokens), tokens))
        return carry

    lax.fori_loop(0, peers, finish_turn, 0)
    own = rows_ref.at[pl.ds(pl.multiple_of(mine * tokens, tokens), tokens), :]
    own_rows = pltpu.make_async_copy(
        own, token_ref.at[:, pl.ds(pl.multiple_of(mine * two, two), two)], own_sem.at[chunks]
    )
    own_rows.start()

    def row_start(q, carry):
        row_copy(q, (mine + q) % peers, mine).start()
        return carry

    lax.fori_loop(1, peers, row_start, 0)

    lax.fori_loop(inside * each, relays, relay, 0)

    def close(chunk, carry):
        own_copy(chunk).wait()

        def shut(hop, inner):
            pair_copy(weight_ref.at[chunk], chunk, mine, hop).wait()
            return inner

        def shut_ring(hop, inner):
            ring_copy(weight_ref.at[chunk], chunk, mine, hop, after).wait_send()
            return inner

        lax.fori_loop(0, ring, shut, 0)
        lax.fori_loop(0, ring - 1, shut_ring, 0)
        return carry

    lax.fori_loop(0, chunks, close, 0)
    own_rows.wait()

    def row_end(q, carry):
        row_copy(q, (mine + q) % peers, (mine + peers - q) % peers).wait()
        return carry

    lax.fori_loop(1, peers, row_end, 0)
    for q in range(1, groups):
        ep_copy(q, here).wait_send()


def mixer_and_weights(
    receptance, key_in, payload_vectors, decay_in, rate_in, gate_in, norm_gain, weights
):
    length, channels = receptance.shape
    groups, peers = lax.axis_size("ep"), lax.axis_size("tp")
    ring = peers // 2
    wide = 2 * HEAD_DIM
    spare = wide - channels
    pad = lambda x: jnp.pad(x, ((0, 0),) * (x.ndim - 1) + ((0, spare),)) if spare else x
    chunks, height, width = weights.shape
    vmem = pl.BlockSpec(memory_space=pltpu.VMEM)
    dma = pltpu.SemaphoreType.DMA
    tokens, whole = pl.pallas_call(
        functools.partial(mixer_kernel, 4, groups, ring),
        out_shape=(
            jax.ShapeDtypeStruct((length // peers, peers * wide), jnp.bfloat16),
            jax.ShapeDtypeStruct((chunks * peers * height, width), jnp.bfloat16),
        ),
        in_specs=[vmem] * 8,
        out_specs=(vmem, pl.BlockSpec(memory_space=pl.ANY)),
        scratch_shapes=[
            pltpu.VMEM((2 * wide, wide), jnp.float32),
            pltpu.VMEM((length, wide), jnp.float32),
            pltpu.VMEM((length, wide), jnp.float32),
            pltpu.VMEM((length, wide), jnp.bfloat16),
            pltpu.VMEM((groups, 2, HEAD_DIM, wide), jnp.bfloat16),
            dma((chunks, ring)),
            dma((chunks, ring)),
            dma((chunks, ring)),
            dma((chunks, ring)),
            dma((groups,)),
            dma((groups,)),
            dma((peers,)),
            dma((peers,)),
            dma((chunks + 1,)),
        ],
        compiler_params=pltpu.CompilerParams(collective_id=0, has_side_effects=True),
        cost_estimate=pl.CostEstimate(
            flops=2 * length * wide * wide * 200, bytes_accessed=32 << 20, transcendentals=0
        ),
    )(
        pad(receptance),
        pad(key_in),
        pad(payload_vectors),
        pad(decay_in),
        pad(rate_in),
        pad(gate_in),
        pad(norm_gain).reshape(1, wide),
        weights,
    )
    if spare:
        tokens = tokens.reshape(-1, peers, wide)[:, :, :channels].reshape(-1, peers * channels)
    return tokens, whole


def silu(x):
    return x / (1.0 + jnp.exp(-x))


def ffn_kernel(x_ref, gate_ref, up_ref, down_ref, out_ref):
    groups, slots, width = x_ref.shape[0], x_ref.shape[2], x_ref.shape[3]
    x = x_ref[...].reshape(groups * slots, width)
    nt = (((1,), (1,)), ((), ()))
    gate = lax.dot_general(x, gate_ref[0], nt, preferred_element_type=jnp.float32)
    upper = lax.dot_general(x, up_ref[0], nt, preferred_element_type=jnp.float32)
    hidden = (silu(gate) * upper).astype(jnp.bfloat16)
    out = jnp.dot(hidden, down_ref[0], preferred_element_type=jnp.float32)
    out_ref[...] = out.astype(jnp.bfloat16).reshape(groups, 1, slots, width)


def expert_layer(
    moe_in,
    moe_gain,
    routes,
    route_weights,
    local_count,
    whole,
    shared_gate,
    shared_up,
    shared_down,
):
    tokens, width = moe_in.shape
    top_count = routes.shape[1]
    groups = lax.axis_size("ep")
    experts = local_count * groups
    slots = max(2, 3 * tokens * top_count // (2 * experts))
    slots = -(-slots // 16) * 16
    values = moe_in.astype(jnp.float32)
    centered = values - jnp.mean(values, -1, keepdims=True)
    rescaled_input = (
        centered * lax.rsqrt(jnp.mean(centered * centered, -1, keepdims=True) + 1e-05) * moe_gain
    ).astype(jnp.bfloat16)
    flat = routes.reshape(-1)
    picks = (flat[:, None] == jnp.arange(experts, dtype=jnp.int32)[None, :]).astype(jnp.int32)
    earlier = jnp.cumsum(picks, axis=0) - picks
    rank = jnp.sum(earlier * picks, axis=1)
    slot_index = (flat * slots + rank).reshape(tokens, top_count)
    total_slots = experts * slots
    slot_row = jnp.arange(total_slots, dtype=jnp.int32)[None, :]
    match = [slot_index[:, k : k + 1] == slot_row for k in range(top_count)]
    chosen = functools.reduce(jnp.logical_or, match).astype(jnp.bfloat16)
    outgoing = lax.dot_general(
        chosen, rescaled_input, (((0,), (0,)), ((), ())), preferred_element_type=jnp.float32
    ).astype(jnp.bfloat16)
    outgoing = outgoing.reshape(groups, local_count * slots, width)
    arrived = lax.all_to_all(outgoing, "ep", split_axis=0, concat_axis=0, tiled=True).reshape(
        groups, local_count, slots, width
    )
    shared_gate_out = jnp.dot(rescaled_input, shared_gate, preferred_element_type=jnp.float32)
    shared_up_out = jnp.dot(rescaled_input, shared_up, preferred_element_type=jnp.float32)
    shared_hidden = (jax.nn.silu(shared_gate_out) * shared_up_out).astype(jnp.bfloat16)
    shared_term = jnp.dot(shared_hidden, shared_down, preferred_element_type=jnp.float32)
    span = whole.shape[1]
    block = (groups, 1, slots, width)
    results = pl.pallas_call(
        ffn_kernel,
        grid=(local_count,),
        out_shape=jax.ShapeDtypeStruct((groups, local_count, slots, width), jnp.bfloat16),
        in_specs=[pl.BlockSpec(block, lambda e: (0, e, 0, 0))]
        + [
            pl.BlockSpec((1, span, width), functools.partial(lambda k, e: (k + e, 0, 0), k))
            for k in (0, local_count, 2 * local_count)
        ],
        out_specs=pl.BlockSpec(block, lambda e: (0, e, 0, 0)),
        cost_estimate=pl.CostEstimate(
            flops=6 * total_slots * width * span, bytes_accessed=16 << 20, transcendentals=0
        ),
    )(arrived, whole, whole, whole)
    sending = results.reshape(groups, local_count * slots, width)
    returned = lax.all_to_all(sending, "ep", split_axis=0, concat_axis=0, tiled=True).reshape(
        total_slots, width
    )
    share = 2.5 * route_weights / jnp.sum(route_weights, -1, keepdims=True)
    spread = sum(jnp.where(match[k], share[:, k : k + 1], 0.0) for k in range(top_count))
    high = spread.astype(jnp.bfloat16)
    low = (spread - high.astype(jnp.float32)).astype(jnp.bfloat16)
    routed = jnp.dot(high, returned, preferred_element_type=jnp.float32) + jnp.dot(
        low, returned, preferred_element_type=jnp.float32
    )
    return (shared_term + routed).astype(jnp.bfloat16)


def project_kernel(rows_ref, weight_ref, out_ref):
    out_ref[...] = jnp.dot(
        rows_ref[...], weight_ref[...], preferred_element_type=jnp.float32
    ).astype(out_ref.dtype)


def shards(
    receptance,
    key_in,
    payload_vectors,
    decay_in,
    rate_in,
    gate_in,
    norm_gain,
    out_weight,
    moe_in,
    moe_gain,
    routes,
    route_weights,
    expert_gate,
    expert_up,
    expert_down,
    shared_gate,
    shared_up,
    shared_down,
):
    local_count, width, part = expert_gate.shape
    weights = jnp.concatenate(
        [jnp.swapaxes(w, 1, 2) for w in (expert_gate, expert_up, expert_down)]
        + [out_weight.reshape(2, part, width)],
        axis=0,
    )
    token_rows, whole = mixer_and_weights(
        receptance, key_in, payload_vectors, decay_in, rate_in, gate_in, norm_gain, weights
    )
    mixed = pl.pallas_call(
        project_kernel,
        grid=(2,),
        out_shape=jax.ShapeDtypeStruct((token_rows.shape[0], width), jnp.bfloat16),
        in_specs=[
            pl.BlockSpec(token_rows.shape, lambda n: (0, 0)),
            pl.BlockSpec((token_rows.shape[1], width // 2), lambda n: (3, n)),
        ],
        out_specs=pl.BlockSpec((token_rows.shape[0], width // 2), lambda n: (0, n)),
        cost_estimate=pl.CostEstimate(
            flops=2 * token_rows.size * width, bytes_accessed=5 << 20, transcendentals=0
        ),
    )(token_rows, whole)
    moe_out = expert_layer(
        moe_in,
        moe_gain,
        routes,
        route_weights,
        local_count,
        whole.reshape(4 * local_count, -1, width),
        shared_gate,
        shared_up,
        shared_down,
    )
    return (mixed, moe_out)


def solution(mesh):
    placed = (
        P("ep", "tp"),
        P("ep", "tp"),
        P("ep", "tp"),
        P("ep", "tp"),
        P("ep", "tp"),
        P("ep", "tp"),
        P("tp"),
        P("tp", None),
        P(("ep", "tp"), None),
        P(),
        P(("ep", "tp"), None),
        P(("ep", "tp"), None),
        P("ep", None, "tp"),
        P("ep", None, "tp"),
        P("ep", None, "tp"),
        P(),
        P(),
        P(),
    )
    return jax.shard_map(
        shards,
        mesh=mesh,
        in_specs=placed,
        out_specs=(P(("ep", "tp"), None), P(("ep", "tp"), None)),
        check_vma=False,
    )
```

```python
import functools

import jax
import jax.numpy as jnp
from jax import lax
from jax.experimental import pallas as pl
from jax.experimental.pallas import tpu as pltpu
from jax.sharding import PartitionSpec as P

HEAD_DIM = 64
BLOCK = 64


def dims(form):
    return {"nn": ((1,), (0,)), "nt": ((1,), (1,)), "tn": ((0,), (0,))}[form]


def mm1(left, right, form="nn"):
    return lax.dot_general(
        left.astype(jnp.bfloat16),
        right.astype(jnp.bfloat16),
        (dims(form), ((), ())),
        preferred_element_type=jnp.float32,
    )


def mm3(left, right, form="nn"):
    lh, rh = left.astype(jnp.bfloat16), right.astype(jnp.bfloat16)
    ll = (left - lh.astype(jnp.float32)).astype(jnp.bfloat16)
    rl = (right - rh.astype(jnp.float32)).astype(jnp.bfloat16)
    return mm1(lh, rh, form) + (mm1(lh, rl, form) + mm1(ll, rh, form))


mm_g = mm3
mm_inv = mm3
mm_q = mm3
mm_out = mm3
mm_car = mm3
mm_scan = mm3


def head_masks(rows, width):
    lane = lax.broadcasted_iota(jnp.int32, (rows, width), 1)
    return lane < HEAD_DIM


def stacked(x):
    first = head_masks(*x.shape)
    return jnp.concatenate([jnp.where(first, x, 0.0), jnp.where(first, 0.0, x)], axis=0)


def per_head_sum(x):
    first = head_masks(*x.shape)
    one = jnp.sum(jnp.where(first, x, 0.0), axis=-1, keepdims=True)
    both = jnp.sum(jnp.where(first, 0.0, x), axis=-1, keepdims=True)
    return jnp.where(first, one, both)


def sigmoid(x):
    return 1.0 / (1.0 + jnp.exp(-x))


def local_block(r_in, k_in, v_in, d_in, b_in):
    f32 = jnp.float32
    keys = k_in.astype(f32)
    unit = keys * lax.rsqrt(per_head_sum(keys * keys) + 1e-06)
    log_decay = sigmoid(d_in.astype(f32)) * -0.6065306597126334
    tri_row = lax.broadcasted_iota(jnp.int32, (BLOCK, 3 * BLOCK), 0)
    tri_col = lax.broadcasted_iota(jnp.int32, (BLOCK, 3 * BLOCK), 1) % BLOCK
    tri = jnp.where(tri_col <= tri_row, 1.0, 0.0).astype(jnp.bfloat16)
    hi = log_decay.astype(jnp.bfloat16)
    rest = log_decay - hi.astype(f32)
    mid = rest.astype(jnp.bfloat16)
    low = (rest - mid.astype(f32)).astype(jnp.bfloat16)
    cumul = mm1(tri, jnp.concatenate([hi, mid, low], axis=0))
    end_scale = jnp.exp(cumul[BLOCK - 1 :, :])
    shrink = jnp.exp(-cumul)
    query2 = stacked(r_in.astype(f32) * jnp.exp(cumul))
    alpha2 = stacked(-unit * jnp.exp(cumul - log_decay))
    key_grow = keys * shrink
    beta_grow = unit * sigmoid(b_in.astype(f32)) * shrink
    values2 = stacked(v_in.astype(f32))
    two = 2 * BLOCK
    grams = mm_g(
        jnp.concatenate([alpha2, query2], axis=0),
        jnp.concatenate([beta_grow, beta_grow, key_grow, key_grow], axis=0),
        "nt",
    )
    row = lax.broadcasted_iota(jnp.int32, (two, two), 0)
    col = lax.broadcasted_iota(jnp.int32, (two, two), 1)
    same = row // BLOCK == col // BLOCK
    strict = same & (col < row)
    inclusive = same & (col <= row)
    couple = jnp.where(strict, grams[:two, :two], 0.0)
    insert = jnp.where(strict, grams[:two, two:], 0.0)
    read_beta = jnp.where(inclusive, grams[two:, :two], 0.0)
    read_key = jnp.where(inclusive, grams[two:, two:], 0.0)
    size = 8
    near = jnp.where(row // size == col // size, couple, 0.0)
    inverse = jnp.where(row == col, 1.0, 0.0) + near
    power = mm_inv(near, near)
    both = mm_inv(jnp.concatenate([inverse, power], axis=0), power)
    inverse = inverse + both[:two]
    inverse = inverse + mm_inv(inverse, both[two:])
    while size < BLOCK:
        wide = 2 * size
        off = jnp.where(
            (row // wide == col // wide) & (row // size != col // size), couple, 0.0
        )
        inverse = inverse + mm_inv(inverse, mm_inv(off, inverse))
        size = wide
    inserted = mm_q(insert, values2)
    qz = mm_q(inverse, jnp.concatenate([alpha2, inserted], axis=1))
    lower = jnp.concatenate([jnp.zeros_like(values2), values2], axis=1)
    stack = jnp.concatenate([qz, lower], axis=0)
    reads = mm_out(jnp.concatenate([read_beta, read_key], axis=1), stack)
    query_bar = query2 + reads[:, :two]
    local_out = reads[:, two:]
    ends = jnp.concatenate([stacked(beta_grow * end_scale), stacked(key_grow * end_scale)], axis=0)
    maps = mm_car(stack, ends, "tn")
    return query_bar, local_out, maps, end_scale


def mixer_kernel(
    unroll,
    groups,
    ring,
    r_ref,
    k_ref,
    v_ref,
    d_ref,
    b_ref,
    gate_ref,
    gain_ref,
    weight_ref,
    slab_ref,
    token_ref,
    whole_ref,
    project_ref,
    state,
    qp_ref,
    lo_ref,
    rows_ref,
    totals,
    ring_send,
    ring_recv,
    pair_send,
    pair_recv,
    ep_send,
    ep_recv,
    row_send,
    row_recv,
    own_sem,
    slab_ring_send,
    slab_ring_recv,
    slab_send,
    slab_recv,
):
    two = 2 * BLOCK
    peers = 2 * ring
    here, mine = lax.axis_index("ep"), lax.axis_index("tp")
    depth, core = mine // 2, mine % 2
    partner = depth * 2 + 1 - core
    after = (depth + 1) % ring * 2 + core
    before = (depth + ring - 1) % ring * 2 + core
    chunks, height = weight_ref.shape[0], weight_ref.shape[1]
    kinds = chunks // 2
    span = peers * height
    tokens = token_ref.shape[0]
    MESH = pl.DeviceIdType.MESH

    def place(chunk, origin):
        base = chunk * span + origin * height
        return whole_ref.at[pl.ds(pl.multiple_of(base, height), height), :]

    def ring_copy(source, chunk, origin, step, target):
        return pltpu.make_async_remote_copy(
            src_ref=source,
            dst_ref=place(chunk, origin),
            send_sem=ring_send.at[chunk, step],
            recv_sem=ring_recv.at[chunk, step],
            device_id={"tp": target},
            device_id_type=MESH,
        )

    def pair_copy(source, chunk, origin, step):
        return pltpu.make_async_remote_copy(
            src_ref=source,
            dst_ref=place(chunk, origin),
            send_sem=pair_send.at[chunk, step],
            recv_sem=pair_recv.at[chunk, step],
            device_id={"tp": partner},
            device_id_type=MESH,
        )

    half, columns = slab_ref.shape[0] // 2, slab_ref.shape[1]

    def slab_place(way, origin):
        return project_ref.at[
            pl.ds(pl.multiple_of(origin * 2 * half + way * half, half), half),
            pl.ds(pl.multiple_of(here * columns, columns), columns),
        ]

    def slab_ring(source, way, origin, step):
        return pltpu.make_async_remote_copy(
            src_ref=source,
            dst_ref=slab_place(way, origin),
            send_sem=slab_ring_send.at[way, step],
            recv_sem=slab_ring_recv.at[way, step],
            device_id={"tp": (after, before)[way]},
            device_id_type=MESH,
        )

    def slab_copies(source, way, origin, step):
        for q in range(groups):
            for flip in (0, 1):
                if q or flip:
                    yield pltpu.make_async_remote_copy(
                        src_ref=source,
                        dst_ref=slab_place(way, origin),
                        send_sem=slab_send.at[way, step, q, flip],
                        recv_sem=slab_recv.at[way, step, q, flip],
                        device_id={
                            "ep": (here + q) % groups,
                            "tp": (mine, partner)[flip],
                        },
                        device_id_type=MESH,
                    )

    def slab_own(way):
        return pltpu.make_async_copy(
            slab_ref.at[pl.ds(way * half, half), :],
            slab_place(way, mine),
            own_sem.at[chunks + 1 + way],
        )

    def slab_relay(hop, carry):
        for way in (0, 1):
            shift = ring - hop if way == 0 else hop
            origin = (depth + shift) % ring * 2 + core
            block = slab_place(way, origin)
            slab_ring(block, way, origin, hop - 1).wait_recv()

            @pl.when(hop < ring - 1)
            def _():
                slab_ring(block, way, origin, hop).start()

            for copy in slab_copies(block, way, origin, hop):
                copy.start()
        return carry

    def own_copy(chunk):
        return pltpu.make_async_copy(
            weight_ref.at[chunk], place(chunk, mine), own_sem.at[chunk]
        )

    barrier = pltpu.get_barrier_semaphore()
    for q in range(1, peers):
        pl.semaphore_signal(
            barrier, inc=1, device_id={"tp": (mine + q) % peers}, device_id_type=MESH
        )
    for q in range(1, groups):
        pl.semaphore_signal(
            barrier, inc=1, device_id={"ep": (here + q) % groups}, device_id_type=MESH
        )
    for q in range(1, groups):
        pl.semaphore_signal(
            barrier,
            inc=1,
            device_id={"ep": (here + q) % groups, "tp": partner},
            device_id_type=MESH,
        )
    pl.semaphore_wait(barrier, peers + 2 * groups - 3)
    for way in (0, 1):
        piece = slab_ref.at[pl.ds(way * half, half), :]
        slab_ring(piece, way, mine, 0).start()
        slab_own(way).start()
        for copy in slab_copies(piece, way, mine, 0):
            copy.start()

    def begin(kind, carry):
        for way, target in ((0, after), (1, before)):
            chunk = kind * 2 + way
            ring_copy(weight_ref.at[chunk], chunk, mine, 0, target).start()
            pair_copy(weight_ref.at[chunk], chunk, mine, 0).start()
            own_copy(chunk).start()
        return carry

    lax.fori_loop(0, kinds, begin, 0)

    def relay(k, carry):
        hop, kind = k // kinds + 1, k % kinds
        for way, target in ((0, after), (1, before)):
            chunk = kind * 2 + way
            shift = ring - hop if way == 0 else hop
            origin = (depth + shift) % ring * 2 + core
            block = place(chunk, origin)
            ring_copy(block, chunk, origin, hop - 1, target).wait_recv()

            @pl.when(hop < ring - 1)
            def _():
                ring_copy(block, chunk, origin, hop, target).start()

            pair_copy(block, chunk, origin, hop).start()
        return carry

    row = lax.broadcasted_iota(jnp.int32, (2 * two, two), 0)
    col = lax.broadcasted_iota(jnp.int32, (2 * two, two), 1)
    state[...] = jnp.where(row == col, 1.0, 0.0)
    turns = r_ref.shape[0] // (BLOCK * unroll)
    relays = (ring - 1) * kinds
    each = 2
    inside = min(turns, relays // each)

    def turn(step, carry):
        parts = []
        for u in range(unroll):
            rows = pl.ds(pl.multiple_of((step * unroll + u) * BLOCK, BLOCK), BLOCK)
            parts.append(
                local_block(
                    r_ref[rows, :], k_ref[rows, :], v_ref[rows, :], d_ref[rows, :], b_ref[rows, :]
                )
            )
        now = state[...]
        for u, (query_bar, local_out, maps, end_scale) in enumerate(parts):
            rows = pl.ds(pl.multiple_of((step * unroll + u) * BLOCK, BLOCK), BLOCK)
            out = mm_scan(query_bar, now, "nt")
            qp_ref[rows, :] = out[:BLOCK, :two] + out[BLOCK:, :two]
            lo = out[:, two:] + local_out
            lo_ref[rows, :] = lo[:BLOCK] + lo[BLOCK:]
            moved = mm_scan(now, maps[:two]) + now * end_scale
            now = jnp.concatenate([moved[:two], moved[two:] + maps[two:]], axis=0)
        state[...] = now

        @pl.when((step >= 1) & (step < ring))
        def _():
            slab_relay(step, 0)

        @pl.when(step < inside)
        def _():
            lax.fori_loop(step * each, (step + 1) * each, relay, 0)

        return carry

    lax.fori_loop(0, turns, turn, 0)

    carry_map, source_map = state[:two, :], state[two:, :]
    totals[here, 0] = (carry_map[:BLOCK] + carry_map[BLOCK:]).astype(totals.dtype)
    totals[here, 1] = (source_map[:BLOCK] + source_map[BLOCK:]).astype(totals.dtype)

    def ep_copy(q, slot):
        return pltpu.make_async_remote_copy(
            src_ref=totals.at[slot],
            dst_ref=totals.at[slot],
            send_sem=ep_send.at[q],
            recv_sem=ep_recv.at[q],
            device_id={"ep": (here + q) % groups},
            device_id_type=MESH,
        )

    for q in range(1, groups):
        ep_copy(q, here).start()
    for q in range(1, groups):
        ep_copy(q, (here + groups - q) % groups).wait_recv()

    def enter(k, entry):
        carry = stacked(totals[k, 0].astype(jnp.float32))
        source = stacked(totals[k, 1].astype(jnp.float32))
        reached = jnp.where(k < here, 1.0, 0.0)
        return entry + reached * (mm3(entry, carry) + source - entry)

    entry = lax.fori_loop(0, groups, enter, jnp.zeros((two, two), jnp.float32))
    entry = entry.astype(jnp.float32)

    def row_copy(q, target, source):
        return pltpu.make_async_remote_copy(
            src_ref=rows_ref.at[pl.ds(pl.multiple_of(target * tokens, tokens), tokens), :],
            dst_ref=token_ref.at[:, pl.ds(pl.multiple_of(source * two, two), two)],
            send_sem=row_send.at[q],
            recv_sem=row_recv.at[q],
            device_id={"tp": target},
            device_id_type=MESH,
        )

    def finish(rows):
        recur = mm3(qp_ref[rows, :], entry, "nt") + lo_ref[rows, :]
        centered = recur - per_head_sum(recur) * (1.0 / HEAD_DIM)
        spread = per_head_sum(centered * centered) * (1.0 / HEAD_DIM)
        normed = centered * lax.rsqrt(spread + 0.00064)
        gated = normed * gain_ref[...] * sigmoid(gate_ref[rows, :].astype(jnp.float32))
        rows_ref[rows, :] = gated.astype(rows_ref.dtype)

    def finish_turn(q, carry):
        target = (mine + q) % peers
        finish(pl.ds(pl.multiple_of(target * tokens, tokens), tokens))
        return carry

    lax.fori_loop(0, peers, finish_turn, 0)
    own = rows_ref.at[pl.ds(pl.multiple_of(mine * tokens, tokens), tokens), :]
    own_rows = pltpu.make_async_copy(
        own, token_ref.at[:, pl.ds(pl.multiple_of(mine * two, two), two)], own_sem.at[chunks]
    )
    own_rows.start()

    def row_start(q, carry):
        row_copy(q, (mine + q) % peers, mine).start()
        return carry

    lax.fori_loop(1, peers, row_start, 0)

    lax.fori_loop(min(turns, ring), ring, slab_relay, 0)
    lax.fori_loop(inside * each, relays, relay, 0)

    def slab_close(hop, carry):
        for way in (0, 1):
            piece = slab_ref.at[pl.ds(way * half, half), :]
            for copy in slab_copies(piece, way, mine, hop):
                copy.wait()

            @pl.when(hop < ring - 1)
            def _():
                slab_ring(piece, way, mine, hop).wait_send()

        return carry

    lax.fori_loop(0, ring, slab_close, 0)
    slab_own(0).wait()
    slab_own(1).wait()

    def close(chunk, carry):
        own_copy(chunk).wait()

        def shut(hop, inner):
            pair_copy(weight_ref.at[chunk], chunk, mine, hop).wait()
            return inner

        def shut_ring(hop, inner):
            ring_copy(weight_ref.at[chunk], chunk, mine, hop, after).wait_send()
            return inner

        lax.fori_loop(0, ring, shut, 0)
        lax.fori_loop(0, ring - 1, shut_ring, 0)
        return carry

    lax.fori_loop(0, chunks, close, 0)
    own_rows.wait()

    def row_end(q, carry):
        row_copy(q, (mine + q) % peers, (mine + peers - q) % peers).wait()
        return carry

    lax.fori_loop(1, peers, row_end, 0)
    for q in range(1, groups):
        ep_copy(q, here).wait_send()


def mixer_and_weights(
    receptance, key_in, payload_vectors, decay_in, rate_in, gate_in, norm_gain, weights, out_weight
):
    length, channels = receptance.shape
    groups, peers = lax.axis_size("ep"), lax.axis_size("tp")
    ring = peers // 2
    wide = 2 * HEAD_DIM
    spare = wide - channels
    pad = lambda x: jnp.pad(x, ((0, 0),) * (x.ndim - 1) + ((0, spare),)) if spare else x
    chunks, height, width = weights.shape
    vmem = pl.BlockSpec(memory_space=pltpu.VMEM)
    dma = pltpu.SemaphoreType.DMA
    columns = width // groups
    slab = lax.dynamic_slice_in_dim(out_weight, lax.axis_index("ep") * columns, columns, axis=1)
    tokens, whole, project = pl.pallas_call(
        functools.partial(mixer_kernel, 4, groups, ring),
        out_shape=(
            jax.ShapeDtypeStruct((length // peers, peers * wide), jnp.bfloat16),
            jax.ShapeDtypeStruct((chunks * peers * height, width), jnp.bfloat16),
            jax.ShapeDtypeStruct((peers * out_weight.shape[0], width), jnp.bfloat16),
        ),
        in_specs=[vmem] * 9,
        out_specs=(vmem, pl.BlockSpec(memory_space=pl.ANY), pl.BlockSpec(memory_space=pl.ANY)),
        scratch_shapes=[
            pltpu.VMEM((2 * wide, wide), jnp.float32),
            pltpu.VMEM((length, wide), jnp.float32),
            pltpu.VMEM((length, wide), jnp.float32),
            pltpu.VMEM((length, wide), jnp.bfloat16),
            pltpu.VMEM((groups, 2, HEAD_DIM, wide), jnp.bfloat16),
            dma((chunks, ring)),
            dma((chunks, ring)),
            dma((chunks, ring)),
            dma((chunks, ring)),
            dma((groups,)),
            dma((groups,)),
            dma((peers,)),
            dma((peers,)),
            dma((chunks + 3,)),
            dma((2, ring)),
            dma((2, ring)),
            dma((2, ring, groups, 2)),
            dma((2, ring, groups, 2)),
        ],
        compiler_params=pltpu.CompilerParams(collective_id=0, has_side_effects=True),
        cost_estimate=pl.CostEstimate(
            flops=2 * length * wide * wide * 200, bytes_accessed=32 << 20, transcendentals=0
        ),
    )(
        pad(receptance),
        pad(key_in),
        pad(payload_vectors),
        pad(decay_in),
        pad(rate_in),
        pad(gate_in),
        pad(norm_gain).reshape(1, wide),
        weights,
        slab,
    )
    if spare:
        tokens = tokens.reshape(-1, peers, wide)[:, :, :channels].reshape(-1, peers * channels)
    return tokens, whole, project


def silu(x):
    return x / (1.0 + jnp.exp(-x))


def ffn_kernel(x_ref, gate_ref, up_ref, down_ref, out_ref):
    groups, slots, width = x_ref.shape[0], x_ref.shape[2], x_ref.shape[3]
    x = x_ref[...].reshape(groups * slots, width)
    nt = (((1,), (1,)), ((), ()))
    gate = lax.dot_general(x, gate_ref[0], nt, preferred_element_type=jnp.float32)
    upper = lax.dot_general(x, up_ref[0], nt, preferred_element_type=jnp.float32)
    hidden = (silu(gate) * upper).astype(jnp.bfloat16)
    out = jnp.dot(hidden, down_ref[0], preferred_element_type=jnp.float32)
    out_ref[...] = out.astype(jnp.bfloat16).reshape(groups, 1, slots, width)


def expert_layer(
    moe_in,
    moe_gain,
    routes,
    route_weights,
    local_count,
    whole,
    shared_gate,
    shared_up,
    shared_down,
):
    tokens, width = moe_in.shape
    top_count = routes.shape[1]
    groups = lax.axis_size("ep")
    experts = local_count * groups
    slots = max(2, 3 * tokens * top_count // (2 * experts))
    slots = -(-slots // 16) * 16
    values = moe_in.astype(jnp.float32)
    centered = values - jnp.mean(values, -1, keepdims=True)
    rescaled_input = (
        centered * lax.rsqrt(jnp.mean(centered * centered, -1, keepdims=True) + 1e-05) * moe_gain
    ).astype(jnp.bfloat16)
    flat = routes.reshape(-1)
    picks = (flat[:, None] == jnp.arange(experts, dtype=jnp.int32)[None, :]).astype(jnp.int32)
    earlier = jnp.cumsum(picks, axis=0) - picks
    rank = jnp.sum(earlier * picks, axis=1)
    slot_index = (flat * slots + rank).reshape(tokens, top_count)
    total_slots = experts * slots
    slot_row = jnp.arange(total_slots, dtype=jnp.int32)[None, :]
    match = [slot_index[:, k : k + 1] == slot_row for k in range(top_count)]
    chosen = functools.reduce(jnp.logical_or, match).astype(jnp.bfloat16)
    outgoing = lax.dot_general(
        chosen, rescaled_input, (((0,), (0,)), ((), ())), preferred_element_type=jnp.float32
    ).astype(jnp.bfloat16)
    outgoing = outgoing.reshape(groups, local_count * slots, width)
    arrived = lax.all_to_all(outgoing, "ep", split_axis=0, concat_axis=0, tiled=True).reshape(
        groups, local_count, slots, width
    )
    shared_gate_out = jnp.dot(rescaled_input, shared_gate, preferred_element_type=jnp.float32)
    shared_up_out = jnp.dot(rescaled_input, shared_up, preferred_element_type=jnp.float32)
    shared_hidden = (jax.nn.silu(shared_gate_out) * shared_up_out).astype(jnp.bfloat16)
    shared_term = jnp.dot(shared_hidden, shared_down, preferred_element_type=jnp.float32)
    span = whole.shape[1]
    block = (groups, 1, slots, width)
    results = pl.pallas_call(
        ffn_kernel,
        grid=(local_count,),
        out_shape=jax.ShapeDtypeStruct((groups, local_count, slots, width), jnp.bfloat16),
        in_specs=[pl.BlockSpec(block, lambda e: (0, e, 0, 0))]
        + [
            pl.BlockSpec((1, span, width), functools.partial(lambda k, e: (k + e, 0, 0), k))
            for k in (0, local_count, 2 * local_count)
        ],
        out_specs=pl.BlockSpec(block, lambda e: (0, e, 0, 0)),
        cost_estimate=pl.CostEstimate(
            flops=6 * total_slots * width * span, bytes_accessed=16 << 20, transcendentals=0
        ),
    )(arrived, whole, whole, whole)
    sending = results.reshape(groups, local_count * slots, width)
    returned = lax.all_to_all(sending, "ep", split_axis=0, concat_axis=0, tiled=True).reshape(
        total_slots, width
    )
    share = 2.5 * route_weights / jnp.sum(route_weights, -1, keepdims=True)
    spread = sum(jnp.where(match[k], share[:, k : k + 1], 0.0) for k in range(top_count))
    high = spread.astype(jnp.bfloat16)
    low = (spread - high.astype(jnp.float32)).astype(jnp.bfloat16)
    routed = jnp.dot(high, returned, preferred_element_type=jnp.float32) + jnp.dot(
        low, returned, preferred_element_type=jnp.float32
    )
    return (shared_term + routed).astype(jnp.bfloat16)


def project_kernel(rows_ref, weight_ref, out_ref):
    out_ref[...] = jnp.dot(
        rows_ref[...], weight_ref[...], preferred_element_type=jnp.float32
    ).astype(out_ref.dtype)


def shards(
    receptance,
    key_in,
    payload_vectors,
    decay_in,
    rate_in,
    gate_in,
    norm_gain,
    out_weight,
    moe_in,
    moe_gain,
    routes,
    route_weights,
    expert_gate,
    expert_up,
    expert_down,
    shared_gate,
    shared_up,
    shared_down,
):
    local_count, width, part = expert_gate.shape
    weights = jnp.concatenate(
        [jnp.swapaxes(w, 1, 2) for w in (expert_gate, expert_up, expert_down)], axis=0
    )
    token_rows, whole, project = mixer_and_weights(
        receptance,
        key_in,
        payload_vectors,
        decay_in,
        rate_in,
        gate_in,
        norm_gain,
        weights,
        out_weight,
    )
    mixed = pl.pallas_call(
        project_kernel,
        grid=(2,),
        out_shape=jax.ShapeDtypeStruct((token_rows.shape[0], width), jnp.bfloat16),
        in_specs=[
            pl.BlockSpec(token_rows.shape, lambda n: (0, 0)),
            pl.BlockSpec((token_rows.shape[1], width // 2), lambda n: (0, n)),
        ],
        out_specs=pl.BlockSpec((token_rows.shape[0], width // 2), lambda n: (0, n)),
        cost_estimate=pl.CostEstimate(
            flops=2 * token_rows.size * width, bytes_accessed=5 << 20, transcendentals=0
        ),
    )(token_rows, project)
    moe_out = expert_layer(
        moe_in,
        moe_gain,
        routes,
        route_weights,
        local_count,
        whole.reshape(3 * local_count, -1, width),
        shared_gate,
        shared_up,
        shared_down,
    )
    return (mixed, moe_out)


def solution(mesh):
    placed = (
        P("ep", "tp"),
        P("ep", "tp"),
        P("ep", "tp"),
        P("ep", "tp"),
        P("ep", "tp"),
        P("ep", "tp"),
        P("tp"),
        P("tp", None),
        P(("ep", "tp"), None),
        P(),
        P(("ep", "tp"), None),
        P(("ep", "tp"), None),
        P("ep", None, "tp"),
        P("ep", None, "tp"),
        P("ep", None, "tp"),
        P(),
        P(),
        P(),
    )
    return jax.shard_map(
        shards,
        mesh=mesh,
        in_specs=placed,
        out_specs=(P(("ep", "tp"), None), P(("ep", "tp"), None)),
        check_vma=False,
    )
```

```python
import functools

import jax
import jax.numpy as jnp
from jax import lax
from jax.experimental import pallas as pl
from jax.experimental.pallas import tpu as pltpu
from jax.sharding import PartitionSpec as P

HEAD_DIM = 64
BLOCK = 64


def dims(form):
    return {"nn": ((1,), (0,)), "nt": ((1,), (1,)), "tn": ((0,), (0,))}[form]


def mm1(left, right, form="nn"):
    return lax.dot_general(
        left.astype(jnp.bfloat16),
        right.astype(jnp.bfloat16),
        (dims(form), ((), ())),
        preferred_element_type=jnp.float32,
    )


def mm3(left, right, form="nn"):
    lh, rh = left.astype(jnp.bfloat16), right.astype(jnp.bfloat16)
    ll = (left - lh.astype(jnp.float32)).astype(jnp.bfloat16)
    rl = (right - rh.astype(jnp.float32)).astype(jnp.bfloat16)
    return mm1(lh, rh, form) + (mm1(lh, rl, form) + mm1(ll, rh, form))


mm_g = mm3
mm_inv = mm3
mm_q = mm3
mm_out = mm3
mm_car = mm3
mm_scan = mm3


def head_masks(rows, width):
    lane = lax.broadcasted_iota(jnp.int32, (rows, width), 1)
    return lane < HEAD_DIM


def stacked(x):
    first = head_masks(*x.shape)
    return jnp.concatenate([jnp.where(first, x, 0.0), jnp.where(first, 0.0, x)], axis=0)


def per_head_sum(x):
    first = head_masks(*x.shape)
    one = jnp.sum(jnp.where(first, x, 0.0), axis=-1, keepdims=True)
    both = jnp.sum(jnp.where(first, 0.0, x), axis=-1, keepdims=True)
    return jnp.where(first, one, both)


def sigmoid(x):
    return 1.0 / (1.0 + jnp.exp(-x))


def local_block(r_in, k_in, v_in, d_in, b_in):
    f32 = jnp.float32
    keys = k_in.astype(f32)
    unit = keys * lax.rsqrt(per_head_sum(keys * keys) + 1e-06)
    log_decay = sigmoid(d_in.astype(f32)) * -0.6065306597126334
    tri_row = lax.broadcasted_iota(jnp.int32, (BLOCK, 3 * BLOCK), 0)
    tri_col = lax.broadcasted_iota(jnp.int32, (BLOCK, 3 * BLOCK), 1) % BLOCK
    tri = jnp.where(tri_col <= tri_row, 1.0, 0.0).astype(jnp.bfloat16)
    hi = log_decay.astype(jnp.bfloat16)
    rest = log_decay - hi.astype(f32)
    mid = rest.astype(jnp.bfloat16)
    low = (rest - mid.astype(f32)).astype(jnp.bfloat16)
    cumul = mm1(tri, jnp.concatenate([hi, mid, low], axis=0))
    end_scale = jnp.exp(cumul[BLOCK - 1 :, :])
    shrink = jnp.exp(-cumul)
    query2 = stacked(r_in.astype(f32) * jnp.exp(cumul))
    alpha2 = stacked(-unit * jnp.exp(cumul - log_decay))
    key_grow = keys * shrink
    beta_grow = unit * sigmoid(b_in.astype(f32)) * shrink
    values2 = stacked(v_in.astype(f32))
    two = 2 * BLOCK
    grams = mm_g(
        jnp.concatenate([alpha2, query2], axis=0),
        jnp.concatenate([beta_grow, beta_grow, key_grow, key_grow], axis=0),
        "nt",
    )
    row = lax.broadcasted_iota(jnp.int32, (two, two), 0)
    col = lax.broadcasted_iota(jnp.int32, (two, two), 1)
    same = row // BLOCK == col // BLOCK
    strict = same & (col < row)
    inclusive = same & (col <= row)
    couple = jnp.where(strict, grams[:two, :two], 0.0)
    insert = jnp.where(strict, grams[:two, two:], 0.0)
    read_beta = jnp.where(inclusive, grams[two:, :two], 0.0)
    read_key = jnp.where(inclusive, grams[two:, two:], 0.0)
    size = 8
    near = jnp.where(row // size == col // size, couple, 0.0)
    inverse = jnp.where(row == col, 1.0, 0.0) + near
    power = mm_inv(near, near)
    both = mm_inv(jnp.concatenate([inverse, power], axis=0), power)
    inverse = inverse + both[:two]
    inverse = inverse + mm_inv(inverse, both[two:])
    while size < BLOCK:
        wide = 2 * size
        off = jnp.where(
            (row // wide == col // wide) & (row // size != col // size), couple, 0.0
        )
        inverse = inverse + mm_inv(inverse, mm_inv(off, inverse))
        size = wide
    inserted = mm_q(insert, values2)
    qz = mm_q(inverse, jnp.concatenate([alpha2, inserted], axis=1))
    lower = jnp.concatenate([jnp.zeros_like(values2), values2], axis=1)
    stack = jnp.concatenate([qz, lower], axis=0)
    reads = mm_out(jnp.concatenate([read_beta, read_key], axis=1), stack)
    query_bar = query2 + reads[:, :two]
    local_out = reads[:, two:]
    ends = jnp.concatenate([stacked(beta_grow * end_scale), stacked(key_grow * end_scale)], axis=0)
    maps = mm_car(stack, ends, "tn")
    return query_bar, local_out, maps, end_scale


def mixer_kernel(
    unroll,
    groups,
    ring,
    r_ref,
    k_ref,
    v_ref,
    d_ref,
    b_ref,
    gate_ref,
    gain_ref,
    weight_ref,
    slab_ref,
    token_ref,
    whole_ref,
    project_ref,
    state,
    qp_ref,
    lo_ref,
    rows_ref,
    totals,
    ring_send,
    ring_recv,
    pair_send,
    pair_recv,
    ep_send,
    ep_recv,
    row_send,
    row_recv,
    own_sem,
    slab_ring_send,
    slab_ring_recv,
    slab_send,
    slab_recv,
):
    two = 2 * BLOCK
    peers = 2 * ring
    here, mine = lax.axis_index("ep"), lax.axis_index("tp")
    depth, core = mine // 2, mine % 2
    partner = depth * 2 + 1 - core
    after = (depth + 1) % ring * 2 + core
    before = (depth + ring - 1) % ring * 2 + core
    chunks, height = weight_ref.shape[0], weight_ref.shape[1]
    kinds = chunks // 2
    span = peers * height
    tokens = token_ref.shape[0]
    MESH = pl.DeviceIdType.MESH

    def place(chunk, origin):
        base = chunk * span + origin * height
        return whole_ref.at[pl.ds(pl.multiple_of(base, height), height), :]

    def ring_copy(source, chunk, origin, step, target):
        return pltpu.make_async_remote_copy(
            src_ref=source,
            dst_ref=place(chunk, origin),
            send_sem=ring_send.at[chunk, step],
            recv_sem=ring_recv.at[chunk, step],
            device_id={"tp": target},
            device_id_type=MESH,
        )

    def pair_copy(source, chunk, origin, step):
        return pltpu.make_async_remote_copy(
            src_ref=source,
            dst_ref=place(chunk, origin),
            send_sem=pair_send.at[chunk, step],
            recv_sem=pair_recv.at[chunk, step],
            device_id={"tp": partner},
            device_id_type=MESH,
        )

    half, columns = slab_ref.shape[0] // 2, slab_ref.shape[1]

    def slab_place(way, origin):
        return project_ref.at[
            pl.ds(pl.multiple_of(origin * 2 * half + way * half, half), half),
            pl.ds(pl.multiple_of(here * columns, columns), columns),
        ]

    def slab_ring(source, way, origin, step):
        return pltpu.make_async_remote_copy(
            src_ref=source,
            dst_ref=slab_place(way, origin),
            send_sem=slab_ring_send.at[way, step],
            recv_sem=slab_ring_recv.at[way, step],
            device_id={"tp": (after, before)[way]},
            device_id_type=MESH,
        )

    def slab_copies(source, way, origin, step):
        for q in range(groups):
            for flip in (0, 1):
                if q or flip:
                    yield pltpu.make_async_remote_copy(
                        src_ref=source,
                        dst_ref=slab_place(way, origin),
                        send_sem=slab_send.at[way, step, q, flip],
                        recv_sem=slab_recv.at[way, step, q, flip],
                        device_id={
                            "ep": (here + q) % groups,
                            "tp": (mine, partner)[flip],
                        },
                        device_id_type=MESH,
                    )

    def slab_own(way):
        return pltpu.make_async_copy(
            slab_ref.at[pl.ds(way * half, half), :],
            slab_place(way, mine),
            own_sem.at[chunks + 1 + way],
        )

    def slab_relay(hop, carry):
        for way in (0, 1):
            shift = ring - hop if way == 0 else hop
            origin = (depth + shift) % ring * 2 + core
            block = slab_place(way, origin)
            slab_ring(block, way, origin, hop - 1).wait_recv()

            @pl.when(hop < ring - 1)
            def _():
                slab_ring(block, way, origin, hop).start()

            for copy in slab_copies(block, way, origin, hop):
                copy.start()
        return carry

    def own_copy(chunk):
        return pltpu.make_async_copy(
            weight_ref.at[chunk], place(chunk, mine), own_sem.at[chunk]
        )

    barrier = pltpu.get_barrier_semaphore()
    for q in range(1, peers):
        pl.semaphore_signal(
            barrier, inc=1, device_id={"tp": (mine + q) % peers}, device_id_type=MESH
        )
    for q in range(1, groups):
        pl.semaphore_signal(
            barrier, inc=1, device_id={"ep": (here + q) % groups}, device_id_type=MESH
        )
    for q in range(1, groups):
        pl.semaphore_signal(
            barrier,
            inc=1,
            device_id={"ep": (here + q) % groups, "tp": partner},
            device_id_type=MESH,
        )
    pl.semaphore_wait(barrier, peers + 2 * groups - 3)
    for way in (0, 1):
        piece = slab_ref.at[pl.ds(way * half, half), :]
        slab_ring(piece, way, mine, 0).start()
        slab_own(way).start()
        for copy in slab_copies(piece, way, mine, 0):
            copy.start()

    def begin(kind, carry):
        for way, target in ((0, after), (1, before)):
            chunk = kind * 2 + way
            ring_copy(weight_ref.at[chunk], chunk, mine, 0, target).start()
            pair_copy(weight_ref.at[chunk], chunk, mine, 0).start()
            own_copy(chunk).start()
        return carry

    lax.fori_loop(0, kinds, begin, 0)

    def relay(k, carry):
        hop, kind = k // kinds + 1, k % kinds
        for way, target in ((0, after), (1, before)):
            chunk = kind * 2 + way
            shift = ring - hop if way == 0 else hop
            origin = (depth + shift) % ring * 2 + core
            block = place(chunk, origin)
            ring_copy(block, chunk, origin, hop - 1, target).wait_recv()

            @pl.when(hop < ring - 1)
            def _():
                ring_copy(block, chunk, origin, hop, target).start()

            pair_copy(block, chunk, origin, hop).start()
        return carry

    row = lax.broadcasted_iota(jnp.int32, (2 * two, two), 0)
    col = lax.broadcasted_iota(jnp.int32, (2 * two, two), 1)
    state[...] = jnp.where(row == col, 1.0, 0.0)
    turns = r_ref.shape[0] // (BLOCK * unroll)
    relays = (ring - 1) * kinds
    each = 1
    inside = min(turns, relays // each)

    def turn(step, carry):
        parts = []
        for u in range(unroll):
            rows = pl.ds(pl.multiple_of((step * unroll + u) * BLOCK, BLOCK), BLOCK)
            parts.append(
                local_block(
                    r_ref[rows, :], k_ref[rows, :], v_ref[rows, :], d_ref[rows, :], b_ref[rows, :]
                )
            )
        now = state[...]
        for u, (query_bar, local_out, maps, end_scale) in enumerate(parts):
            rows = pl.ds(pl.multiple_of((step * unroll + u) * BLOCK, BLOCK), BLOCK)
            out = mm_scan(query_bar, now, "nt")
            qp_ref[rows, :] = out[:BLOCK, :two] + out[BLOCK:, :two]
            lo = out[:, two:] + local_out
            lo_ref[rows, :] = lo[:BLOCK] + lo[BLOCK:]
            moved = mm_scan(now, maps[:two]) + now * end_scale
            now = jnp.concatenate([moved[:two], moved[two:] + maps[two:]], axis=0)
        state[...] = now

        @pl.when((step >= 1) & (step < ring))
        def _():
            slab_relay(step, 0)

        @pl.when(step < inside)
        def _():
            lax.fori_loop(step * each, (step + 1) * each, relay, 0)

        return carry

    lax.fori_loop(0, turns, turn, 0)

    carry_map, source_map = state[:two, :], state[two:, :]
    totals[here, 0] = (carry_map[:BLOCK] + carry_map[BLOCK:]).astype(totals.dtype)
    totals[here, 1] = (source_map[:BLOCK] + source_map[BLOCK:]).astype(totals.dtype)

    def ep_copy(q, slot):
        return pltpu.make_async_remote_copy(
            src_ref=totals.at[slot],
            dst_ref=totals.at[slot],
            send_sem=ep_send.at[q],
            recv_sem=ep_recv.at[q],
            device_id={"ep": (here + q) % groups},
            device_id_type=MESH,
        )

    for q in range(1, groups):
        ep_copy(q, here).start()
    for q in range(1, groups):
        ep_copy(q, (here + groups - q) % groups).wait_recv()

    def enter(k, entry):
        carry = stacked(totals[k, 0].astype(jnp.float32))
        source = stacked(totals[k, 1].astype(jnp.float32))
        reached = jnp.where(k < here, 1.0, 0.0)
        return entry + reached * (mm3(entry, carry) + source - entry)

    entry = lax.fori_loop(0, groups, enter, jnp.zeros((two, two), jnp.float32))
    entry = entry.astype(jnp.float32)

    def row_copy(q, target, source):
        return pltpu.make_async_remote_copy(
            src_ref=rows_ref.at[pl.ds(pl.multiple_of(target * tokens, tokens), tokens), :],
            dst_ref=token_ref.at[:, pl.ds(pl.multiple_of(source * two, two), two)],
            send_sem=row_send.at[q],
            recv_sem=row_recv.at[q],
            device_id={"tp": target},
            device_id_type=MESH,
        )

    def finish(rows):
        recur = mm3(qp_ref[rows, :], entry, "nt") + lo_ref[rows, :]
        centered = recur - per_head_sum(recur) * (1.0 / HEAD_DIM)
        spread = per_head_sum(centered * centered) * (1.0 / HEAD_DIM)
        normed = centered * lax.rsqrt(spread + 0.00064)
        gated = normed * gain_ref[...] * sigmoid(gate_ref[rows, :].astype(jnp.float32))
        rows_ref[rows, :] = gated.astype(rows_ref.dtype)

    def finish_turn(q, carry):
        target = (mine + q) % peers
        finish(pl.ds(pl.multiple_of(target * tokens, tokens), tokens))
        return carry

    lax.fori_loop(0, peers, finish_turn, 0)
    own = rows_ref.at[pl.ds(pl.multiple_of(mine * tokens, tokens), tokens), :]
    own_rows = pltpu.make_async_copy(
        own, token_ref.at[:, pl.ds(pl.multiple_of(mine * two, two), two)], own_sem.at[chunks]
    )
    own_rows.start()

    def row_start(q, carry):
        row_copy(q, (mine + q) % peers, mine).start()
        return carry

    lax.fori_loop(1, peers, row_start, 0)

    lax.fori_loop(min(turns, ring), ring, slab_relay, 0)
    lax.fori_loop(inside * each, relays, relay, 0)

    def slab_close(hop, carry):
        for way in (0, 1):
            piece = slab_ref.at[pl.ds(way * half, half), :]
            for copy in slab_copies(piece, way, mine, hop):
                copy.wait()

            @pl.when(hop < ring - 1)
            def _():
                slab_ring(piece, way, mine, hop).wait_send()

        return carry

    lax.fori_loop(0, ring, slab_close, 0)
    slab_own(0).wait()
    slab_own(1).wait()

    def close(chunk, carry):
        own_copy(chunk).wait()

        def shut(hop, inner):
            pair_copy(weight_ref.at[chunk], chunk, mine, hop).wait()
            return inner

        def shut_ring(hop, inner):
            ring_copy(weight_ref.at[chunk], chunk, mine, hop, after).wait_send()
            return inner

        lax.fori_loop(0, ring, shut, 0)
        lax.fori_loop(0, ring - 1, shut_ring, 0)
        return carry

    lax.fori_loop(0, chunks, close, 0)
    own_rows.wait()

    def row_end(q, carry):
        row_copy(q, (mine + q) % peers, (mine + peers - q) % peers).wait()
        return carry

    lax.fori_loop(1, peers, row_end, 0)
    for q in range(1, groups):
        ep_copy(q, here).wait_send()


def mixer_and_weights(
    receptance, key_in, payload_vectors, decay_in, rate_in, gate_in, norm_gain, weights, out_weight
):
    length, channels = receptance.shape
    groups, peers = lax.axis_size("ep"), lax.axis_size("tp")
    ring = peers // 2
    wide = 2 * HEAD_DIM
    spare = wide - channels
    pad = lambda x: jnp.pad(x, ((0, 0),) * (x.ndim - 1) + ((0, spare),)) if spare else x
    chunks, height, width = weights.shape
    vmem = pl.BlockSpec(memory_space=pltpu.VMEM)
    dma = pltpu.SemaphoreType.DMA
    columns = width // groups
    slab = lax.dynamic_slice_in_dim(out_weight, lax.axis_index("ep") * columns, columns, axis=1)
    tokens, whole, project = pl.pallas_call(
        functools.partial(mixer_kernel, 4, groups, ring),
        out_shape=(
            jax.ShapeDtypeStruct((length // peers, peers * wide), jnp.bfloat16),
            jax.ShapeDtypeStruct((chunks * peers * height, width), jnp.bfloat16),
            jax.ShapeDtypeStruct((peers * out_weight.shape[0], width), jnp.bfloat16),
        ),
        in_specs=[vmem] * 9,
        out_specs=(vmem, pl.BlockSpec(memory_space=pl.ANY), pl.BlockSpec(memory_space=pl.ANY)),
        scratch_shapes=[
            pltpu.VMEM((2 * wide, wide), jnp.float32),
            pltpu.VMEM((length, wide), jnp.float32),
            pltpu.VMEM((length, wide), jnp.float32),
            pltpu.VMEM((length, wide), jnp.bfloat16),
            pltpu.VMEM((groups, 2, HEAD_DIM, wide), jnp.bfloat16),
            dma((chunks, ring)),
            dma((chunks, ring)),
            dma((chunks, ring)),
            dma((chunks, ring)),
            dma((groups,)),
            dma((groups,)),
            dma((peers,)),
            dma((peers,)),
            dma((chunks + 3,)),
            dma((2, ring)),
            dma((2, ring)),
            dma((2, ring, groups, 2)),
            dma((2, ring, groups, 2)),
        ],
        compiler_params=pltpu.CompilerParams(collective_id=0, has_side_effects=True),
        cost_estimate=pl.CostEstimate(
            flops=2 * length * wide * wide * 200, bytes_accessed=32 << 20, transcendentals=0
        ),
    )(
        pad(receptance),
        pad(key_in),
        pad(payload_vectors),
        pad(decay_in),
        pad(rate_in),
        pad(gate_in),
        pad(norm_gain).reshape(1, wide),
        weights,
        slab,
    )
    if spare:
        tokens = tokens.reshape(-1, peers, wide)[:, :, :channels].reshape(-1, peers * channels)
    return tokens, whole, project


def silu(x):
    return x / (1.0 + jnp.exp(-x))


def ffn_kernel(x_ref, gate_ref, up_ref, down_ref, out_ref):
    groups, slots, width = x_ref.shape[0], x_ref.shape[2], x_ref.shape[3]
    x = x_ref[...].reshape(groups * slots, width)
    nt = (((1,), (1,)), ((), ()))
    gate = lax.dot_general(x, gate_ref[0], nt, preferred_element_type=jnp.float32)
    upper = lax.dot_general(x, up_ref[0], nt, preferred_element_type=jnp.float32)
    hidden = (silu(gate) * upper).astype(jnp.bfloat16)
    out = jnp.dot(hidden, down_ref[0], preferred_element_type=jnp.float32)
    out_ref[...] = out.astype(jnp.bfloat16).reshape(groups, 1, slots, width)


def expert_layer(
    moe_in,
    moe_gain,
    routes,
    route_weights,
    local_count,
    whole,
    shared_gate,
    shared_up,
    shared_down,
):
    tokens, width = moe_in.shape
    top_count = routes.shape[1]
    groups = lax.axis_size("ep")
    experts = local_count * groups
    slots = max(2, 3 * tokens * top_count // (2 * experts))
    slots = -(-slots // 16) * 16
    values = moe_in.astype(jnp.float32)
    centered = values - jnp.mean(values, -1, keepdims=True)
    rescaled_input = (
        centered * lax.rsqrt(jnp.mean(centered * centered, -1, keepdims=True) + 1e-05) * moe_gain
    ).astype(jnp.bfloat16)
    flat = routes.reshape(-1)
    picks = (flat[:, None] == jnp.arange(experts, dtype=jnp.int32)[None, :]).astype(jnp.int32)
    earlier = jnp.cumsum(picks, axis=0) - picks
    rank = jnp.sum(earlier * picks, axis=1)
    slot_index = (flat * slots + rank).reshape(tokens, top_count)
    total_slots = experts * slots
    slot_row = jnp.arange(total_slots, dtype=jnp.int32)[None, :]
    match = [slot_index[:, k : k + 1] == slot_row for k in range(top_count)]
    chosen = functools.reduce(jnp.logical_or, match).astype(jnp.bfloat16)
    outgoing = lax.dot_general(
        chosen, rescaled_input, (((0,), (0,)), ((), ())), preferred_element_type=jnp.float32
    ).astype(jnp.bfloat16)
    outgoing = outgoing.reshape(groups, local_count * slots, width)
    arrived = lax.all_to_all(outgoing, "ep", split_axis=0, concat_axis=0, tiled=True).reshape(
        groups, local_count, slots, width
    )
    shared_gate_out = jnp.dot(rescaled_input, shared_gate, preferred_element_type=jnp.float32)
    shared_up_out = jnp.dot(rescaled_input, shared_up, preferred_element_type=jnp.float32)
    shared_hidden = (jax.nn.silu(shared_gate_out) * shared_up_out).astype(jnp.bfloat16)
    shared_term = jnp.dot(shared_hidden, shared_down, preferred_element_type=jnp.float32)
    span = whole.shape[1]
    block = (groups, 1, slots, width)
    results = pl.pallas_call(
        ffn_kernel,
        grid=(local_count,),
        out_shape=jax.ShapeDtypeStruct((groups, local_count, slots, width), jnp.bfloat16),
        in_specs=[pl.BlockSpec(block, lambda e: (0, e, 0, 0))]
        + [
            pl.BlockSpec((1, span, width), functools.partial(lambda k, e: (k + e, 0, 0), k))
            for k in (0, local_count, 2 * local_count)
        ],
        out_specs=pl.BlockSpec(block, lambda e: (0, e, 0, 0)),
        cost_estimate=pl.CostEstimate(
            flops=6 * total_slots * width * span, bytes_accessed=16 << 20, transcendentals=0
        ),
    )(arrived, whole, whole, whole)
    sending = results.reshape(groups, local_count * slots, width)
    returned = lax.all_to_all(sending, "ep", split_axis=0, concat_axis=0, tiled=True).reshape(
        total_slots, width
    )
    share = 2.5 * route_weights / jnp.sum(route_weights, -1, keepdims=True)
    spread = sum(jnp.where(match[k], share[:, k : k + 1], 0.0) for k in range(top_count))
    high = spread.astype(jnp.bfloat16)
    low = (spread - high.astype(jnp.float32)).astype(jnp.bfloat16)
    routed = jnp.dot(high, returned, preferred_element_type=jnp.float32) + jnp.dot(
        low, returned, preferred_element_type=jnp.float32
    )
    return (shared_term + routed).astype(jnp.bfloat16)


def project_kernel(rows_ref, weight_ref, out_ref):
    out_ref[...] = jnp.dot(
        rows_ref[...], weight_ref[...], preferred_element_type=jnp.float32
    ).astype(out_ref.dtype)


def shards(
    receptance,
    key_in,
    payload_vectors,
    decay_in,
    rate_in,
    gate_in,
    norm_gain,
    out_weight,
    moe_in,
    moe_gain,
    routes,
    route_weights,
    expert_gate,
    expert_up,
    expert_down,
    shared_gate,
    shared_up,
    shared_down,
):
    local_count, width, part = expert_gate.shape
    weights = jnp.concatenate(
        [jnp.swapaxes(w, 1, 2) for w in (expert_gate, expert_up, expert_down)], axis=0
    )
    token_rows, whole, project = mixer_and_weights(
        receptance,
        key_in,
        payload_vectors,
        decay_in,
        rate_in,
        gate_in,
        norm_gain,
        weights,
        out_weight,
    )
    mixed = pl.pallas_call(
        project_kernel,
        grid=(2,),
        out_shape=jax.ShapeDtypeStruct((token_rows.shape[0], width), jnp.bfloat16),
        in_specs=[
            pl.BlockSpec(token_rows.shape, lambda n: (0, 0)),
            pl.BlockSpec((token_rows.shape[1], width // 2), lambda n: (0, n)),
        ],
        out_specs=pl.BlockSpec((token_rows.shape[0], width // 2), lambda n: (0, n)),
        cost_estimate=pl.CostEstimate(
            flops=2 * token_rows.size * width, bytes_accessed=5 << 20, transcendentals=0
        ),
    )(token_rows, project)
    moe_out = expert_layer(
        moe_in,
        moe_gain,
        routes,
        route_weights,
        local_count,
        whole.reshape(3 * local_count, -1, width),
        shared_gate,
        shared_up,
        shared_down,
    )
    return (mixed, moe_out)


def solution(mesh):
    placed = (
        P("ep", "tp"),
        P("ep", "tp"),
        P("ep", "tp"),
        P("ep", "tp"),
        P("ep", "tp"),
        P("ep", "tp"),
        P("tp"),
        P("tp", None),
        P(("ep", "tp"), None),
        P(),
        P(("ep", "tp"), None),
        P(("ep", "tp"), None),
        P("ep", None, "tp"),
        P("ep", None, "tp"),
        P("ep", None, "tp"),
        P(),
        P(),
        P(),
    )
    return jax.shard_map(
        shards,
        mesh=mesh,
        in_specs=placed,
        out_specs=(P(("ep", "tp"), None), P(("ep", "tp"), None)),
        check_vma=False,
    )
```
